32 devices in a mesh: fs: 8 (over z, y), tp: 4 (over x, core).
Axes of the slice: x: 2, y: 2, z: 4, core: 2. Of those that a mesh axis runs over, the one named last changes fastest.
Arguments:
- tokens: bfloat16 [4096, 4096], P('fs'), may hold values from -6 to 6
- norm_gain: float32 [4096], P('fs'), may hold values from 0.1 to 1.9
- gate_train: float32 [8, 4096, 1024], P(None, 'fs', 'tp'), may hold values from -0.09375 to 0.09375
- up_train: float32 [8, 4096, 1024], P(None, 'fs', 'tp'), may hold values from -0.09375 to 0.09375
- down_train: float32 [8, 1024, 4096], P(None, 'fs', 'tp'), may hold values from -0.1875 to 0.1875
- shared_gate_train: float32 [4096, 1024], P('fs', 'tp'), may hold values from -0.09375 to 0.09375
- shared_up_train: float32 [4096, 1024], P('fs', 'tp'), may hold values from -0.09375 to 0.09375
- shared_down_train: float32 [1024, 4096], P('fs', 'tp'), may hold values from -0.1875 to 0.1875
- route_expert: int32 [4096, 2], P('fs'), may hold values from 0 to 7, all different within a row; in each aligned block of 512 rows (0 to 511, 512 to 1023, ...) at most 192 rows name the same one
- route_weight: float32 [4096, 2], P('fs'), may hold values from 0.1 to 1
Outputs:
- expert_gate: bfloat16 [8, 4096, 1024], P('fs', None, 'tp')
- expert_up: bfloat16 [8, 4096, 1024], P('fs', None, 'tp')
- expert_down: bfloat16 [8, 1024, 4096], P('fs', 'tp')
- shared_gate: bfloat16 [4096, 1024], P(None, 'tp')
- shared_up: bfloat16 [4096, 1024], P(None, 'tp')
- shared_down: bfloat16 [1024, 4096], P('tp')
- mixed: bfloat16 [4096, 4096], P('fs', 'tp')
The draws below stay inside these ranges and needn't reach their ends.
Inputs may be any that keep to these rules, and one draw needn't show every extreme that they name: `route_expert`: each row names 2 different experts. Within each aligned block of 512 rows no expert is named by more than 192 rows, a bound that some block reaches in every draw.
All inputs are finite; a program needn't handle non-finite values.
Results may differ from the reference program's by a relative error of at most 0.015.
Values may be sent and summed in bfloat16 or wider, within the bound.
A program may use at most 128 MiB of HBM per device.

```python
import math
import jax
import jax.numpy as jnp
import numpy as np
from jax import lax

D = 4096
H = 1024
HS = 1024
TOPK = 2
TOK_DEV = 512
EXPERTS = 8
CAP = 192
TOKENS = 4096
N_FS = 8
N_TP = 4


def levels(rng, dims, shards, low, top_value):
    loudness = 1.0
    for axis_at, shards_of in shards:
        draws = jax.random.uniform(jax.random.fold_in(jax.random.fold_in(rng, 6), axis_at), (shards_of,), jnp.float32, low / len(shards), top_value / len(shards))
        loudness = loudness * jnp.repeat(jnp.exp(draws), dims[axis_at] // shards_of).reshape((-1,) + (1,) * (len(dims) - 1 - axis_at))
    return loudness


def shared_out(key, own, number, rows, amount, top, reach, lean):
    sequence = jax.random.permutation(key, amount)
    crowded, ordinary = shares(amount, rows * top, reach, lean, True), shares(amount, rows * top, reach, lean, False)
    places = jnp.arange(amount)

    def named(sizes, rotation):
        used = int((sizes > 0).sum())
        fixed = max(1, used // 4)
        shifted = fixed + (places - fixed + rotation * (used - fixed)) % max(1, amount - fixed)
        return jnp.zeros((amount,), jnp.int32).at[sequence[jnp.where(places < fixed, places, shifted)]].set(jnp.asarray(sizes, jnp.int32))

    sizes = jnp.where(number % 4 == 0, named(crowded, number // 4), named(ordinary, number - number // 4 - 1))
    mixed = jax.random.permutation(jax.random.fold_in(own, 3), amount)
    giver, taker = mixed[0:amount // 2 * 2:2], mixed[1:amount // 2 * 2:2]
    margin = jnp.minimum(sizes[giver] - 1, reach - sizes[taker]) // 2
    margin = jnp.where((giver == sequence[0]) | (taker == sequence[0]) | (sizes[taker] == 0), 0, jnp.maximum(margin, 0))
    shifted = jax.random.randint(jax.random.fold_in(own, 4), (amount // 2,), 0, 1 << 20) % (margin + 1)
    sizes = sizes.at[giver].add(-shifted).at[taker].add(shifted)
    labels = jnp.searchsorted(jnp.cumsum(sizes), jnp.arange(rows * top), side="right").astype(jnp.int32)
    table = labels.reshape(top, rows).T
    table = table[jax.random.permutation(jax.random.fold_in(own, 1), rows)]
    rotation = jax.random.randint(jax.random.fold_in(own, 2), (rows, 1), 0, top)
    return jnp.take_along_axis(table, (jnp.arange(top)[None, :] + rotation) % top, axis=1)


def shares(amount, total, reach, skew, full):
    portions = [(1 << 20) // math.isqrt(standing ** skew) + 1 for standing in range(1, amount + 1)]
    largest = reach if full else min(reach, max(-(-total // amount), total * portions[0] // sum(portions)))
    least = 1 if total - largest >= amount - 1 else 0
    holding, surplus = [largest] + [least] * (amount - 1), total - largest - least * (amount - 1)
    while surplus > 0:
        free = [i for i in range(1, amount) if holding[i] < largest] or [i for i in range(1, amount) if holding[i] < reach]
        whole, left = sum([portions[i] for i in free]), surplus
        for i in free:
            more = min(reach - holding[i], max(1, left * portions[i] // whole), surplus)
            holding[i] = holding[i] + more
            surplus = surplus - more
    return np.array(holding)


def noise(own_key, extent, spread, limit, shards=(), kind=jnp.bfloat16):
    loudness = levels(own_key, extent, shards, -0.22, 0.18) if shards else 1.0
    array = jax.random.normal(own_key, extent, jnp.float32) * spread * loudness
    return jnp.minimum(jnp.maximum(array, -limit), limit).astype(kind)


def setup_inputs(seed: int = 0) -> dict:
    keys = jax.random.split(jax.random.key(seed), 11)
    tokens = noise(keys[0], (TOKENS, D), 1.0, 6.0, ((0, 8),))
    norm_gain = jnp.clip(1.0 + 0.18 * jax.random.normal(keys[1], (D,), jnp.float32), 0.1, 1.9)
    gate_train = noise(keys[2], (EXPERTS, D, H), D ** -0.5, 0.09375, ((1, 8), (2, 4)), jnp.float32)
    up_train = noise(keys[3], (EXPERTS, D, H), D ** -0.5, 0.09375, ((1, 8), (2, 4)), jnp.float32)
    down_train = noise(keys[4], (EXPERTS, H, D), H ** -0.5, 0.1875, ((1, 8), (2, 4)), jnp.float32)
    shared_gate_train = noise(keys[5], (D, HS), D ** -0.5, 0.09375, ((0, 8), (1, 4)), jnp.float32)
    shared_up_train = noise(keys[6], (D, HS), D ** -0.5, 0.09375, ((0, 8), (1, 4)), jnp.float32)
    shared_down_train = noise(keys[7], (HS, D), HS ** -0.5, 0.1875, ((0, 8), (1, 4)), jnp.float32)
    route_expert_keys = jax.random.split(jax.random.fold_in(keys[8], 1), TOKENS // TOK_DEV)
    route_expert_turns = jax.random.permutation(jax.random.fold_in(keys[8], 3), TOKENS // TOK_DEV)
    route_expert = jax.vmap(lambda own, number: shared_out(jax.random.fold_in(keys[8], 2), own, number, TOK_DEV, EXPERTS, TOPK, CAP, 1))(route_expert_keys, route_expert_turns).reshape((TOKENS, TOPK))
    route_weight = jnp.clip(jnp.exp(math.log(1.0) - 2.3025851 * jax.random.uniform(keys[9], (TOKENS, TOPK), jnp.float32) ** levels(keys[9], (TOKENS, TOPK), ((0, 8),), -0.2, 0.2)), 0.1, 1.0)
    return {"tokens": tokens, "norm_gain": norm_gain, "gate_train": gate_train, "up_train": up_train, "down_train": down_train, "shared_gate_train": shared_gate_train, "shared_up_train": shared_up_train, "shared_down_train": shared_down_train, "route_expert": route_expert, "route_weight": route_weight}


norm_eps = 1e-06

def expert_apply(rows, weight_gate, weight_up, weight_down, pieces):
    gate_vals = jnp.dot(rows, weight_gate, preferred_element_type=jnp.float32)
    up_vals = jnp.dot(rows, weight_up, preferred_element_type=jnp.float32)
    hidden = (jax.nn.silu(gate_vals) * up_vals).astype(jnp.bfloat16)
    step_width = hidden.shape[1] // pieces
    total = jnp.zeros((rows.shape[0], weight_down.shape[1]), jnp.float32)
    for block in range(pieces):
        term = jnp.dot(hidden[:, block * step_width:(block + 1) * step_width], weight_down[block * step_width:(block + 1) * step_width], preferred_element_type=jnp.float32)
        total = total + term.astype(jnp.bfloat16).astype(jnp.float32)
    return total

def reference(tokens, norm_gain, gate_train, up_train, down_train, shared_gate_train, shared_up_train, shared_down_train, route_expert, route_weight):
    expert_gate = (norm_gain[None, :, None] * gate_train).astype(jnp.bfloat16)
    expert_up = (norm_gain[None, :, None] * up_train).astype(jnp.bfloat16)
    expert_down = down_train.astype(jnp.bfloat16)
    shared_gate = (norm_gain[:, None] * shared_gate_train).astype(jnp.bfloat16)
    shared_up = (norm_gain[:, None] * shared_up_train).astype(jnp.bfloat16)
    shared_down = shared_down_train.astype(jnp.bfloat16)
    values = tokens.astype(jnp.float32)
    normed = (values * lax.rsqrt(lax.optimization_barrier(jnp.mean(values * values, axis=1, keepdims=True)) + norm_eps)).astype(jnp.bfloat16)
    pairs = route_expert.reshape(N_FS, TOK_DEV * TOPK)
    chosen = (pairs[:, :, None] == jnp.arange(EXPERTS, dtype=jnp.int32)[None, None, :]).astype(jnp.int32)
    earlier = (jnp.cumsum(chosen, axis=1) - chosen).astype(jnp.int32)
    slot = lax.optimization_barrier(jnp.sum(earlier * chosen, axis=2)).astype(jnp.int32)
    place = (jnp.arange(N_FS, dtype=jnp.int32)[:, None] * CAP + slot).reshape(-1).astype(jnp.int32)
    expert_flat = route_expert.reshape(-1).astype(jnp.int32)
    token_of = (jnp.arange(TOKENS * TOPK, dtype=jnp.int32) // TOPK).astype(jnp.int32)
    table = jnp.zeros((EXPERTS, N_FS * CAP), jnp.int32).at[expert_flat, place].set(token_of)

    def one_expert(operands):
        row_index, weight_gate, weight_up, weight_down = operands
        rows = normed[row_index]
        return expert_apply(rows, weight_gate, weight_up, weight_down, N_TP).astype(jnp.bfloat16)
    results = lax.map(one_expert, (table, expert_gate, expert_up, expert_down))
    picked = results[expert_flat, place].reshape(TOKENS, TOPK, D)
    routed = lax.optimization_barrier(jnp.sum(route_weight[:, :, None] * picked.astype(jnp.float32), axis=1))
    shared_result = expert_apply(normed, shared_gate, shared_up, shared_down, N_TP)
    mixed = (routed + shared_result).astype(jnp.bfloat16)
    return (expert_gate, expert_up, expert_down, shared_gate, shared_up, shared_down, mixed)
```

```python
import functools

import jax
import jax.numpy as jnp
from jax import lax
from jax.experimental import pallas as pl
from jax.experimental.pallas import tpu as pltpu
from jax.sharding import PartitionSpec as P

norm_eps = 1e-06
cores = 2
MESH = pl.DeviceIdType.MESH
F32, BF16 = jnp.float32, jnp.bfloat16


class Sizes:
    def __init__(self, experts, pieces, tokens, gate, down, sgate, sdown, top):
        self.E, self.P = experts, pieces
        self.C = pieces // cores
        long = 1
        while long * long < experts:
            long *= 2
        self.Z, self.Y = long, experts // long
        self.half = experts // 2
        self.T, self.D = tokens
        self.cap = 3 * self.T * top // (2 * experts)
        self.Dr, self.Hc = gate[1:]
        self.Hr, self.Dc = down[1:]
        self.Dr2, self.Sc = sgate
        self.Sr = sdown[0]
        self.per = experts // pieces
        self.g = 1
        while self.g * self.cap % 128:
            self.g *= 2
        self.groups = experts // self.g
        self.M = self.g * self.cap
        self.nt = min(256, self.Dc)


def kernel(
    S,
    tokens, gate_t, up_t, down_t, sgate_t, sup_t, sdown_t, gain, rows_of, cols_of,
    eg, eu, ed, sg, su, sd, mixed,
    nrm, tok, info, shb, sdb, gst, gub, dst, dnb, rows, yst, hid, res, ret, acc, shid, outb,
    wbuf, dbuf,
    ld_sem, tk_ld, out_sem,
    tok_s, tok_r, info_s, info_r, sh_s, sh_r, shy_s, sd_s, sd_r, sdy_s,
    gu_s, gu_r, dn_s, dn_r, y_s, rows_r, x_s, part_s, part_r,
    hid_s, hid_r, shid_s, shid_r, edo_s, edo_r, sdo_s, sdo_r, ret_s, ret_r,
):
    E, Pn, C, Z, Y, half, per = S.E, S.P, S.C, S.Z, S.Y, S.half, S.per
    cap, Dc, Hc, Sc, nt = S.cap, S.Dc, S.Hc, S.Sc, S.nt
    f, t = lax.axis_index("fs"), lax.axis_index("tp")
    z, y = f // Y, f % Y
    x, c = t // cores, t % cores
    h, fo = f // half, f % half

    def ring(k, count, at, back=False):
        mid = count // 2
        far = k // mid
        off = k % mid + far
        side = (at // mid + 1 + far) % 2
        step = at % mid - off + count if back else at % mid + off
        return side * mid + step % mid

    def peer(k):
        return ring(k, E, f)

    def source(k):
        return ring(k, E, f, True)

    def rcopy(src, dst, ssem, rsem, to):
        return pltpu.make_async_remote_copy(
            src_ref=src, dst_ref=dst, send_sem=ssem, recv_sem=rsem,
            device_id=to, device_id_type=MESH,
        )

    def arrived(ref, rsem):
        rcopy(ref, ref, out_sem.at[0], rsem, ((f + 1) % E, t)).wait_recv()

    def sent(ref, ssem):
        rcopy(ref, ref, ssem, out_sem.at[0], ((f + 1) % E, t)).wait_send()

    def loop(count, body, start=0):
        lax.fori_loop(start, count, lambda i, v: (body(i), v)[1], 0)

    def load_w(k, slot):
        e = peer(k)
        return [
            pltpu.make_async_copy(w.at[e], wbuf.at[slot, i], ld_sem.at[slot, i])
            for i, w in ((0, gate_t), (1, up_t))
        ]

    def load_d(k, slot):
        return pltpu.make_async_copy(down_t.at[peer(k)], dbuf.at[slot], ld_sem.at[slot, 2])

    tok_load = pltpu.make_async_copy(tokens, nrm, tk_ld.at[0])
    tok_load.start()
    sh_loads = [
        pltpu.make_async_copy(sgate_t, wbuf.at[1, 0], ld_sem.at[1, 0]),
        pltpu.make_async_copy(sup_t, wbuf.at[1, 1], ld_sem.at[1, 1]),
        pltpu.make_async_copy(sdown_t, dbuf.at[1], ld_sem.at[1, 2]),
    ]
    for copy in sh_loads + load_w(0, 0) + [load_d(0, 0)]:
        copy.start()

    T = S.T
    wide = max(16, E)
    r0, r1 = rows_of[0:1, :], rows_of[1:2, :]
    names = lax.broadcasted_iota(jnp.int32, (wide, T), 0).astype(F32)
    hit0, hit1 = r0 == names, r1 == names
    chosen = (hit0 | hit1).astype(F32).astype(BF16)
    before = lax.broadcasted_iota(jnp.int32, (T, T), 0) < lax.broadcasted_iota(
        jnp.int32, (T, T), 1
    )
    count = jnp.dot(chosen, before.astype(F32).astype(BF16), preferred_element_type=F32)
    s0 = jnp.sum(jnp.where(hit0, count, 0.0), axis=0, keepdims=True)
    s1 = jnp.sum(jnp.where(hit1, count, 0.0), axis=0, keepdims=True)
    info[z, 0:1, :] = r0
    info[z, 1:2, :] = r1
    info[z, 2:3, :] = s0
    info[z, 3:4, :] = s1

    tok_load.wait()
    tile = min(64, T)

    def normalise(i):
        at = pl.ds(pl.multiple_of(i * tile, tile), tile)
        v = nrm[at, :].astype(F32)
        v = v * lax.rsqrt(jnp.mean(v * v, axis=1, keepdims=True) + norm_eps)
        nrm[at, :] = v.astype(BF16)
        tok[z, at, :] = nrm[at, pl.ds(pl.multiple_of(t * Dc, Dc), Dc)]

    loop(T // tile, normalise)

    for copy in sh_loads:
        copy.wait()
    shb[f, :, 0:Sc] = (gain[...] * wbuf[1, 0]).astype(BF16)
    shb[f, :, Sc:] = (gain[...] * wbuf[1, 1]).astype(BF16)
    sdb[f] = dbuf[1].astype(BF16)

    def line(buf, slot_of, ssem, rsem, hop):
        for d, ok_next in ((0, z + 1 < Z), (1, z > 0)):
            zs = z - hop if d == 0 else z + hop
            there = (zs >= 0) if d == 0 else (zs < Z)
            slot = slot_of(jnp.clip(zs, 0, Z - 1))
            nxt = (f + Y if d == 0 else f - Y, t)

            @pl.when(there)
            def _():
                if hop:
                    arrived(buf.at[slot], rsem.at[slot])

                @pl.when(ok_next)
                def _():
                    rcopy(
                        buf.at[slot], buf.at[slot], ssem.at[d, hop], rsem.at[slot], nxt
                    ).start()

    def line_drain(buf, slot_of, ssem):
        for hop in range(Z - 1):
            for d, ok_next in ((0, z + 1 < Z), (1, z > 0)):
                zs = z - hop if d == 0 else z + hop
                there = (zs >= 0) if d == 0 else (zs < Z)
                slot = slot_of(jnp.clip(zs, 0, Z - 1))

                @pl.when(there & ok_next)
                def _():
                    sent(buf.at[slot], ssem.at[d, hop])

    by_z = lambda zs: zs
    by_f = lambda zs: zs * Y + y

    for i in range(1, Z):
        zo = (z + i) % Z
        rcopy(info.at[z], info.at[z], info_s.at[i - 1], info_r.at[z], (zo * Y + y, t)).start()
    line(tok, by_z, tok_s, tok_r, 0)

    def convert_gu(k):
        slot = k % 2
        for copy in load_w(k, slot):
            copy.wait()

        @pl.when(k + 1 < E)
        def _():
            for copy in load_w(k + 1, 1 - slot):
                copy.start()

        for i in range(2):
            gst[k, :, i * Hc : (i + 1) * Hc] = (gain[...] * wbuf[slot, i]).astype(BF16)

    def convert_dn(k):
        slot = k % 2
        load_d(k, slot).wait()

        @pl.when(k + 1 < E)
        def _():
            load_d(k + 1, 1 - slot).start()

        dst[k] = dbuf[slot].astype(BF16)

    loop(E, convert_gu)

    def shared_y(zs):
        s = by_f(zs)
        for j in range(1, Y):
            to = (z * Y + (y + j) % Y, t)
            rcopy(shb.at[s], shb.at[s], shy_s.at[j - 1], sh_r.at[s], to).start()
            rcopy(sdb.at[s], sdb.at[s], sdy_s.at[j - 1], sd_r.at[s], to).start()

    line(shb, by_f, sh_s, sh_r, 0)
    line(sdb, by_f, sd_s, sd_r, 0)
    shared_y(z)
    loop(E, convert_dn)
    gub[f] = gst[E - 1]
    dnb[f] = dst[E - 1]

    def x_out(s):
        for i in range(1, C):
            to = (f, (x + i) % C * cores + c)
            rcopy(rows.at[t, s], rows.at[t, s], x_s.at[i - 1], rows_r.at[t, s], to).start()
        rcopy(rows.at[t, s], rows.at[t, s], part_s.at[0], part_r.at[0], (f, x * cores + 1 - c)).start()

    def pick(zs):
        s = by_f(zs)
        for j in list(range(1, Y)) + [0]:
            e = (z * Y + (y + j) % Y).astype(F32)
            slots = lax.broadcasted_iota(jnp.int32, (cap, T), 0).astype(F32)
            got = (info[zs, 0:1, :] == e) & (info[zs, 2:3, :] == slots)
            got |= (info[zs, 1:2, :] == e) & (info[zs, 3:4, :] == slots)
            got = got.astype(F32).astype(BF16)

            def part(n):
                at = pl.ds(pl.multiple_of(n * nt, nt), nt)
                block = jnp.dot(got, tok[zs, :, at], preferred_element_type=F32).astype(BF16)
                if j:
                    yst[zs, j - 1, :, at] = block
                else:
                    rows[t, s, :, at] = block

            loop(Dc // nt, part)
        for j in range(1, Y):
            to = (z * Y + (y + j) % Y, t)
            rcopy(
                yst.at[zs, j - 1], rows.at[t, s], y_s.at[j - 1], rows_r.at[t, s], to
            ).start()
        x_out(s)

    pick(z)

    def send_gu(k):
        e = peer(k)
        rcopy(gst.at[k], gub.at[f], gu_s.at[k], gu_r.at[f], (e, t)).start()

    def send_dn(k):
        e = peer(k)
        rcopy(dst.at[k], dnb.at[f], dn_s.at[k], dn_r.at[f], (e, t)).start()

    def arrivals(hop):
        for zs, there in ((z - hop, z - hop >= 0), (z + hop, z + hop < Z)):
            at = jnp.clip(zs, 0, Z - 1)

            @pl.when(there)
            def _():
                shared_y(at)
                arrived(info.at[at], info_r.at[at])
                pick(at)

    for hop in range(1, Z):
        line(tok, by_z, tok_s, tok_r, hop)
        line(shb, by_f, sh_s, sh_r, hop)
        line(sdb, by_f, sd_s, sd_r, hop)
        if hop == 1:
            loop(half, send_gu)
        if hop == Z - 2 or Z <= 2:
            loop(E - 1, send_gu, half)
            loop(E - 1, send_dn)
        arrivals(hop)

    for j in range(1, Y):
        for zs in range(Z):
            s = zs * Y + (y + j) % Y
            arrived(rows.at[t, s], rows_r.at[t, s])
            x_out(s)
    for i in range(1, C):
        to_t = (x + i) % C * cores + c

        def forward(s):
            arrived(rows.at[to_t, s], rows_r.at[to_t, s])
            rcopy(
                rows.at[to_t, s], rows.at[to_t, s], part_s.at[i], part_r.at[i],
                (f, x * cores + 1 - c),
            ).start()

        loop(E, forward)

    for j in range(1, Y):
        for zs in range(Z):
            s = zs * Y + (y + j) % Y
            arrived(shb.at[s], sh_r.at[s])
            arrived(sdb.at[s], sd_r.at[s])

    def put(src, dst_ref, i):
        copy = pltpu.make_async_copy(src, dst_ref, out_sem.at[i])
        copy.start()
        return copy

    puts = [put(shb.at[:, :, pl.ds(0, Sc)], sg, 1), put(shb.at[:, :, pl.ds(Sc, Sc)], su, 2)]
    own_cols = pl.ds(pl.multiple_of(t * Dc, Dc), Dc)

    def spread(buf, out, ssem, rsem, i):
        for k in range(1, Pn):
            tt = (t + k) % Pn
            rcopy(
                buf.at[pl.ds(tt * per, per)], out.at[:, :, own_cols], ssem.at[k - 1],
                rsem.at[t], (f, tt),
            ).start()
        return put(buf.at[pl.ds(t * per, per)], out.at[:, :, own_cols], i)

    def spread_wait(buf, out, ssem, rsem):
        for k in range(1, Pn):
            tt = (t + k) % Pn
            sent(buf.at[pl.ds(tt * per, per)], ssem.at[k - 1])
            at = pl.ds(pl.multiple_of(tt * Dc, Dc), Dc)
            arrived(out.at[:, :, at], rsem.at[tt])

    puts.append(spread(sdb, sd, sdo_s, sdo_r, 3))

    def act(v, width):
        gate, up = v[:, :width], v[:, width:]
        return (gate / (1.0 + jnp.exp(-gate)) * up).astype(BF16)

    mt = min(256, T)

    def shared_in(m):
        at = pl.ds(pl.multiple_of(m * mt, mt), mt)
        total = None
        for q in range(Pn):
            w = shb[q * per : (q + 1) * per].reshape(Dc, 2 * Sc)
            term = jnp.dot(nrm[at, q * Dc : (q + 1) * Dc], w, preferred_element_type=F32)
            total = term if total is None else total + term
        shid[t, at, :] = act(total, Sc)

    loop(T // mt, shared_in)

    def rows_waits():
        part = x * cores + 1 - c
        arrived(rows.at[part], part_r.at[0])
        for i in range(1, C):
            arrived(rows.at[(x + i) % C * cores + 1 - c], part_r.at[i])

    rows_waits()
    for k in range(1, Pn):
        rcopy(shid.at[t], shid.at[t], shid_s.at[k - 1], shid_r.at[t], (f, (t + k) % Pn)).start()
    for k in range(1, Pn):
        arrived(shid.at[(t + k) % Pn], shid_r.at[(t + k) % Pn])

    def shared_out(n):
        at = pl.ds(pl.multiple_of(n * nt, nt), nt)
        total = None
        for q in range(Pn):
            w = sdb[q * per : (q + 1) * per, :, at].reshape(Sc, nt)
            term = jnp.dot(shid[q], w, preferred_element_type=F32)
            total = term if total is None else total + term
        acc[:, at] = total

    loop(Dc // nt, shared_out)

    def wait_gu(k):
        s = source(k)
        arrived(gub.at[s], gu_r.at[s])

    loop(E - 1, wait_gu)
    puts.append(put(gub.at[:, :, pl.ds(0, Hc)], eg, 4))
    puts.append(put(gub.at[:, :, pl.ds(Hc, Hc)], eu, 5))
    M, g, groups = S.M, S.g, S.groups
    own = f // g

    def group_at(k):
        return ring(k, groups, own) if groups > 1 else 0

    def hidden_in(k):
        q0 = group_at(k)
        span = pl.ds(q0 * g, g)
        total = None
        for q in range(Pn):
            w = gub[q * per : (q + 1) * per].reshape(Dc, 2 * Hc)
            term = jnp.dot(rows[q, span].reshape(M, Dc), w, preferred_element_type=F32)
            total = term if total is None else total + term
        hid[t, span] = act(total, Hc).reshape(g, cap, Hc)

    def send_hidden(k):
        span = pl.ds(group_at(k) * g, g)
        for j in range(1, Pn):
            tt = (t + j) % Pn
            rcopy(
                hid.at[t, span], hid.at[t, span], hid_s.at[j - 1], hid_r.at[t, k], (f, tt)
            ).start()

    def hidden_step(k):
        hidden_in(k)

        @pl.when(k > 0)
        def _():
            send_hidden(k - 1)

    loop(groups, hidden_step)

    def wait_dn(k):
        s = source(k)
        arrived(dnb.at[s], dn_r.at[s])

    send_hidden(groups - 1)
    loop(E - 1, wait_dn)
    puts.append(spread(dnb, ed, edo_s, edo_r, 6))

    def send_back(k):
        for i in range(g):
            s = group_at(k) * g + i

            @pl.when(s != f)
            def _():
                rcopy(res.at[s], ret.at[f], ret_s.at[s], ret_r.at[f], (s, t)).start()

    def back_step(k):
        span = pl.ds(group_at(k) * g, g)
        for j in range(1, Pn):
            tt = (t + j) % Pn
            arrived(hid.at[tt, span], hid_r.at[tt, k])

        def part(n):
            at = pl.ds(pl.multiple_of(n * nt, nt), nt)
            total = None
            for q in range(Pn):
                w = dnb[q * per : (q + 1) * per, :, at].reshape(Hc, nt)
                term = jnp.dot(hid[q, span].reshape(M, Hc), w, preferred_element_type=F32)
                total = term if total is None else total + term
            res[span, :, at] = total.astype(BF16).reshape(g, cap, nt)

        loop(Dc // nt, part)
        send_back(k)

    loop(groups, back_step)
    ret[f] = res[f]

    def slot_cols(k):
        return jnp.sum(jnp.where(cols_of[:, k : k + 1] == name_cols, count_cols, 0.0), axis=1, keepdims=True)

    name_cols = lax.broadcasted_iota(jnp.int32, (T, 128), 1).astype(F32)
    chosen_cols = ((cols_of[:, 0:1] == name_cols) | (cols_of[:, 1:2] == name_cols)).astype(F32)
    after = lax.broadcasted_iota(jnp.int32, (T, T), 0) > lax.broadcasted_iota(
        jnp.int32, (T, T), 1
    )
    count_cols = jnp.dot(
        after.astype(F32).astype(BF16), chosen_cols.astype(BF16), preferred_element_type=F32
    )
    target0 = cols_of[:, 0:1] * cap + slot_cols(0)
    target1 = cols_of[:, 1:2] * cap + slot_cols(1)
    w0, w1 = cols_of[:, 2:3], cols_of[:, 3:4]

    def combine(i):
        q0 = group_at(groups - 1 - i)
        for j in range(g):
            s = q0 * g + j

            @pl.when(s != f)
            def _():
                arrived(ret.at[s], ret_r.at[s])

        spot = (lax.broadcasted_iota(jnp.int32, (T, M), 1) + q0 * M).astype(F32)
        weigh = jnp.where(target0 == spot, w0, 0.0) + jnp.where(target1 == spot, w1, 0.0)
        weigh = weigh.astype(BF16)

        def part(n):
            at = pl.ds(pl.multiple_of(n * nt, nt), nt)
            block = ret[pl.ds(q0 * g, g), :, at].reshape(M, nt)
            total = acc[:, at] + jnp.dot(weigh, block, preferred_element_type=F32)
            acc[:, at] = total

        loop(Dc // nt, part)

    loop(groups, combine)
    outb[...] = acc[...].astype(BF16)
    puts.append(put(outb, mixed, 7))

    line_drain(tok, by_z, tok_s)
    line_drain(shb, by_f, sh_s)
    line_drain(sdb, by_f, sd_s)
    for i in range(1, Z):
        sent(info.at[z], info_s.at[i - 1])
    for j in range(1, Y):
        sent(shb.at[pl.ds(0, Z)], shy_s.at[j - 1])
        sent(sdb.at[pl.ds(0, Z)], sdy_s.at[j - 1])
        sent(yst.at[:, j - 1], y_s.at[j - 1])
    for i in range(1, C):
        sent(rows.at[t], x_s.at[i - 1])
    for i in range(C):
        sent(rows.at[t], part_s.at[i])
    loop(E - 1, lambda k: sent(gst.at[k], gu_s.at[k]))
    loop(E - 1, lambda k: sent(dst.at[k], dn_s.at[k]))
    for k in range(1, Pn):
        sent(shid.at[t], shid_s.at[k - 1])
        sent(hid.at[t], hid_s.at[k - 1])

    def drain_ret(k):
        s = source(k)
        sent(res.at[s], ret_s.at[s])

    loop(E - 1, drain_ret)
    spread_wait(sdb, sd, sdo_s, sdo_r)
    spread_wait(dnb, ed, edo_s, edo_r)
    for copy in puts:
        copy.wait()


def on_device(
    tokens, norm_gain, gate_train, up_train, down_train,
    shared_gate_train, shared_up_train, shared_down_train, route_expert, route_weight,
):
    S = Sizes(
        lax.axis_size("fs"), lax.axis_size("tp"), tokens.shape, gate_train.shape,
        down_train.shape, shared_gate_train.shape, shared_down_train.shape,
        route_expert.shape[1],
    )
    E, Pn, C, Z, Y = S.E, S.P, S.C, S.Z, S.Y
    T, D, cap, Dr, Hc, Hr, Dc, Sc, Sr, per = (
        S.T, S.D, S.cap, S.Dr, S.Hc, S.Hr, S.Dc, S.Sc, S.Sr, S.per
    )
    route = route_expert.astype(F32)
    columns = jnp.concatenate([route, route_weight], axis=1)
    dma = pltpu.SemaphoreType.DMA
    anywhere = pl.BlockSpec(memory_space=pl.ANY)
    inside = pl.BlockSpec(memory_space=pltpu.VMEM)
    far = max(1, Y - 1)
    scratch = [
        pltpu.VMEM((T, D), BF16),
        pltpu.VMEM((Z, T, Dc), BF16),
        pltpu.VMEM((Z, 8, T), F32),
        pltpu.VMEM((E, Dr, 2 * Sc), BF16),
        pltpu.VMEM((E, Sr, Dc), BF16),
        pltpu.VMEM((E, Dr, 2 * Hc), BF16),
        pltpu.VMEM((E, Dr, 2 * Hc), BF16),
        pltpu.VMEM((E, Hr, Dc), BF16),
        pltpu.VMEM((E, Hr, Dc), BF16),
        pltpu.VMEM((Pn, E, cap, Dc), BF16),
        pltpu.VMEM((Z, far, cap, Dc), BF16),
        pltpu.VMEM((Pn, E, cap, Hc), BF16),
        pltpu.VMEM((E, cap, Dc), BF16),
        pltpu.VMEM((E, cap, Dc), BF16),
        pltpu.VMEM((T, Dc), F32),
        pltpu.VMEM((Pn, T, Sc), BF16),
        pltpu.VMEM((T, Dc), BF16),
        pltpu.VMEM((2, 2, Dr, Hc), F32),
        pltpu.VMEM((2, Hr, Dc), F32),
        dma((2, 3)), dma((1,)), dma((8,)),
        dma((2, Z)), dma((Z,)), dma((Z,)), dma((Z,)),
        dma((2, Z)), dma((E,)), dma((far,)),
        dma((2, Z)), dma((E,)), dma((far,)),
        dma((E,)), dma((E,)), dma((E,)), dma((E,)),
        dma((far,)), dma((Pn, E)), dma((C,)), dma((C,)), dma((C,)),
        dma((Pn,)), dma((Pn, S.groups)), dma((Pn,)), dma((Pn,)),
        dma((Pn,)), dma((Pn,)), dma((Pn,)), dma((Pn,)),
        dma((E,)), dma((E,)),
    ]
    shape = lambda *dims: jax.ShapeDtypeStruct(dims, BF16)
    flops = 2 * T * D * 2 * Sc + 2 * E * cap * D * 2 * Hc + 4 * E * cap * D * Hc
    outs = pl.pallas_call(
        functools.partial(kernel, S),
        out_shape=[
            shape(E, Dr, Hc), shape(E, Dr, Hc), shape(per, Hr, D),
            shape(E, Dr, Sc), shape(E, Dr, Sc), shape(per, Sr, D), shape(T, Dc),
        ],
        in_specs=[anywhere] * 7 + [inside] * 3,
        out_specs=[anywhere] * 7,
        scratch_shapes=scratch,
        compiler_params=pltpu.CompilerParams(
            has_side_effects=True, vmem_limit_bytes=67043328
        ),
        cost_estimate=pl.CostEstimate(flops=flops, bytes_accessed=1 << 26, transcendentals=0),
    )(
        tokens, gate_train, up_train, down_train, shared_gate_train, shared_up_train,
        shared_down_train, norm_gain[:, None], route.T, columns,
    )
    eg, eu, ed, sg, su, sd, mixed = outs
    return (
        eg.reshape(1, D, Hc), eu.reshape(1, D, Hc), ed.reshape(1, per * Hr, D),
        sg.reshape(D, Sc), su.reshape(D, Sc), sd.reshape(per * Sr, D), mixed,
    )


def solution(mesh):
    placed = (
        P("fs", None),
        P("fs"),
        P(None, "fs", "tp"),
        P(None, "fs", "tp"),
        P(None, "fs", "tp"),
        P("fs", "tp"),
        P("fs", "tp"),
        P("fs", "tp"),
        P("fs", None),
        P("fs", None),
    )
    return jax.shard_map(
        on_device,
        mesh=mesh,
        in_specs=placed,
        out_specs=(
            P("fs", None, "tp"),
            P("fs", None, "tp"),
            P("fs", "tp", None),
            P(None, "tp"),
            P(None, "tp"),
            P("tp", None),
            P("fs", "tp"),
        ),
        check_vma=False,
    )
```

```python
import functools

import jax
import jax.numpy as jnp
from jax import lax
from jax.experimental import pallas as pl
from jax.experimental.pallas import tpu as pltpu
from jax.sharding import PartitionSpec as P

norm_eps = 1e-06
cores = 2
MESH = pl.DeviceIdType.MESH
F32, BF16 = jnp.float32, jnp.bfloat16


class Sizes:
    def __init__(self, experts, pieces, tokens, gate, down, sgate, sdown, top):
        self.E, self.P = experts, pieces
        self.C = pieces // cores
        long = 1
        while long * long < experts:
            long *= 2
        self.Z, self.Y = long, experts // long
        self.half = experts // 2
        self.T, self.D = tokens
        self.cap = 3 * self.T * top // (2 * experts)
        self.Dr, self.Hc = gate[1:]
        self.Hr, self.Dc = down[1:]
        self.Dr2, self.Sc = sgate
        self.Sr = sdown[0]
        self.per = experts // pieces
        self.g = 1
        while self.g * self.cap % 128:
            self.g *= 2
        self.groups = experts // self.g
        self.M = self.g * self.cap
        self.nt = min(256, self.Dc)


def kernel(
    S,
    tokens, gate_t, up_t, down_t, sgate_t, sup_t, sdown_t, gain, route, weight,
    eg, eu, ed, sg, su, sd, mixed,
    nrm, tok, info, shb, sdb, gst, gub, dst, dnb, rows, yst, est, hid, res, ret, acc, shid, outb,
    wbuf, dbuf, gcol,
    ld_sem, tk_ld, out_sem,
    tok_s, tok_r, info_s, info_r, sh_s, sh_r, shy_s, sd_s, sd_r, sdy_s,
    gu_s, gu_r, dn_s, dn_r, y_s, e_s, rows_r, x_s, part_s, part_r,
    hid_s, hid_r, shid_s, shid_r, edo_s, edo_r, sdo_s, sdo_r, ret_s, ret_r,
):
    E, Pn, C, Z, Y, half, per = S.E, S.P, S.C, S.Z, S.Y, S.half, S.per
    cap, Dc, Hc, Sc, nt = S.cap, S.Dc, S.Hc, S.Sc, S.nt
    f, t = lax.axis_index("fs"), lax.axis_index("tp")
    z, y = f // Y, f % Y
    x, c = t // cores, t % cores
    inner = (z > 0) & (z < Z - 1)
    to_low, to_high = z == 1, z == Z - 2

    def ring(k, count, at, back=False):
        mid = count // 2
        far = k // mid
        off = k % mid + far
        side = (at // mid + 1 + far) % 2
        step = at % mid - off + count if back else at % mid + off
        return side * mid + step % mid

    def peer(k):
        return ring(k, E, f)

    def source(k):
        return ring(k, E, f, True)

    def rcopy(src, dst, ssem, rsem, to):
        return pltpu.make_async_remote_copy(
            src_ref=src, dst_ref=dst, send_sem=ssem, recv_sem=rsem,
            device_id=to, device_id_type=MESH,
        )

    def arrived(ref, rsem):
        rcopy(ref, ref, out_sem.at[0], rsem, ((f + 1) % E, t)).wait_recv()

    def sent(ref, ssem):
        rcopy(ref, ref, ssem, out_sem.at[0], ((f + 1) % E, t)).wait_send()

    def loop(count, body, start=0):
        lax.fori_loop(start, count, lambda i, v: (body(i), v)[1], 0)

    def load_w(k, slot):
        e = peer(k)
        return [
            pltpu.make_async_copy(w.at[e], wbuf.at[slot, i], ld_sem.at[slot, i])
            for i, w in ((0, gate_t), (1, up_t))
        ]

    def load_d(k, slot):
        return pltpu.make_async_copy(down_t.at[peer(k)], dbuf.at[slot], ld_sem.at[slot, 2])

    tok_load = pltpu.make_async_copy(tokens, nrm, tk_ld.at[0])
    tok_load.start()
    sh_loads = [
        pltpu.make_async_copy(sgate_t, wbuf.at[1, 0], ld_sem.at[1, 0]),
        pltpu.make_async_copy(sup_t, wbuf.at[1, 1], ld_sem.at[1, 1]),
        pltpu.make_async_copy(sdown_t, dbuf.at[1], ld_sem.at[1, 2]),
    ]
    for copy in sh_loads + load_w(0, 0) + [load_d(0, 0)]:
        copy.start()
    greet = pltpu.get_barrier_semaphore()
    for i in range(1, E):
        pl.semaphore_signal(greet, inc=1, device_id=((f + i) % E, t), device_id_type=MESH)
    for i in range(1, Pn):
        pl.semaphore_signal(greet, inc=1, device_id=(f, (t + i) % Pn), device_id_type=MESH)

    T = S.T
    wide = max(16, E)
    gcol[...] = jnp.broadcast_to(gain[...], (128, S.Dr)).T
    lanes = lax.broadcasted_iota(jnp.int32, (T, 128), 1)
    routes = route[...].astype(F32)
    named0, named1 = routes[:, 0:1], routes[:, 1:2]
    by_row = jnp.where(lanes == 0, named0, named1).T
    r0, r1 = by_row[0:1, :], by_row[1:2, :]
    names = lax.broadcasted_iota(jnp.int32, (wide, T), 0).astype(F32)
    hit0, hit1 = r0 == names, r1 == names
    chosen = (hit0 | hit1).astype(F32).astype(BF16)
    before = lax.broadcasted_iota(jnp.int32, (T, T), 0) < lax.broadcasted_iota(
        jnp.int32, (T, T), 1
    )
    count = jnp.dot(chosen, before.astype(F32).astype(BF16), preferred_element_type=F32)
    s0 = jnp.sum(jnp.where(hit0, count, 0.0), axis=0, keepdims=True)
    s1 = jnp.sum(jnp.where(hit1, count, 0.0), axis=0, keepdims=True)
    info[z, 0:1, :] = r0
    info[z, 1:2, :] = r1
    info[z, 2:3, :] = s0
    info[z, 3:4, :] = s1

    tok_load.wait()
    tile = min(64, T)

    def normalise(i):
        at = pl.ds(pl.multiple_of(i * tile, tile), tile)
        v = nrm[at, :].astype(F32)
        v = v * lax.rsqrt(jnp.mean(v * v, axis=1, keepdims=True) + norm_eps)
        nrm[at, :] = v.astype(BF16)
        tok[z, at, :] = nrm[at, pl.ds(pl.multiple_of(t * Dc, Dc), Dc)]

    loop(T // tile, normalise)

    for copy in sh_loads:
        copy.wait()
    shb[f, :, 0:Sc] = (gcol[:, 0:1] * wbuf[1, 0]).astype(BF16)
    shb[f, :, Sc:] = (gcol[:, 0:1] * wbuf[1, 1]).astype(BF16)
    sdb[f] = dbuf[1].astype(BF16)

    by_z = lambda zs: zs
    by_f = lambda zs: zs * Y + y

    pl.semaphore_wait(greet, E + Pn - 2)

    def lanes_of(slot_of, hop, within):
        low, high = (1, Z - 1) if within else (0, Z)
        for d in range(2):
            zs = z - hop if d == 0 else z + hop
            there = (zs >= 0) if d == 0 else (zs < Z)
            if within and hop:
                there &= inner
            onward = (z + 1 < high) if d == 0 else (z > low)
            yield d, there, onward, slot_of(jnp.clip(zs, 0, Z - 1)), f + Y if d == 0 else f - Y

    def line(buf, slot_of, ssem, rsem, hop, within=False):
        for d, there, onward, slot, nxt in lanes_of(slot_of, hop, within):

            @pl.when(there)
            def _():
                if hop:
                    arrived(buf.at[slot], rsem.at[slot])

                @pl.when(onward)
                def _():
                    rcopy(
                        buf.at[slot], buf.at[slot], ssem.at[d, hop], rsem.at[slot], (nxt, t)
                    ).start()

    def line_sent(buf, slot_of, ssem, hop, within=False):
        for d, there, onward, slot, nxt in lanes_of(slot_of, hop, within):

            @pl.when(there & onward)
            def _():
                sent(buf.at[slot], ssem.at[d, hop])

    def tell(act_on):
        for i in range(1, Z):
            zo = (z + i) % Z

            @pl.when((zo > 0) & (zo < Z - 1))
            def _():
                act_on(i - 1, zo)

    tell(
        lambda i, zo: rcopy(
            info.at[z], info.at[z], info_s.at[i], info_r.at[z], (zo * Y + y, t)
        ).start()
    )
    line(tok, by_z, tok_s, tok_r, 0, True)

    def convert_gu(k):
        slot = k % 2
        for copy in load_w(k, slot):
            copy.wait()

        @pl.when(k + 1 < E)
        def _():
            for copy in load_w(k + 1, 1 - slot):
                copy.start()

        for i in range(2):
            gst[k, :, i * Hc : (i + 1) * Hc] = (gcol[:, 0:1] * wbuf[slot, i]).astype(BF16)

    def convert_dn(k):
        slot = k % 2
        load_d(k, slot).wait()

        @pl.when(k + 1 < E)
        def _():
            load_d(k + 1, 1 - slot).start()

        dst[k] = dbuf[slot].astype(BF16)

    def shared_y(zs):
        s = by_f(zs)
        for j in range(1, Y):
            to = (z * Y + (y + j) % Y, t)
            rcopy(shb.at[s], shb.at[s], shy_s.at[j - 1], sh_r.at[s], to).start()
            rcopy(sdb.at[s], sdb.at[s], sdy_s.at[j - 1], sd_r.at[s], to).start()

    def x_out(s):
        for i in range(1, C):
            to = (f, (x + i) % C * cores + c)
            rcopy(rows.at[t, s], rows.at[t, s], x_s.at[i - 1], rows_r.at[t, s], to).start()
        rcopy(rows.at[t, s], rows.at[t, s], part_s.at[0], part_r.at[0], (f, x * cores + 1 - c)).start()

    def picked(zs, e, put_block):
        e = e.astype(F32)
        slots = lax.broadcasted_iota(jnp.int32, (cap, T), 0).astype(F32)
        got = (info[zs, 0:1, :] == e) & (info[zs, 2:3, :] == slots)
        got |= (info[zs, 1:2, :] == e) & (info[zs, 3:4, :] == slots)
        got = got.astype(F32).astype(BF16)

        def part(n):
            at = pl.ds(pl.multiple_of(n * nt, nt), nt)
            put_block(at, jnp.dot(got, tok[zs, :, at], preferred_element_type=F32).astype(BF16))

        loop(Dc // nt, part)

    def pick(zs):
        s = by_f(zs)

        def for_end(zt):
            for j in range(Y):

                def put_block(at, block):
                    est[zs, j, :, at] = block

                picked(zs, zt * Y + (y + j) % Y, put_block)
            for j in range(Y):
                rcopy(
                    est.at[zs, j], rows.at[t, s], e_s.at[j], rows_r.at[t, s],
                    (zt * Y + (y + j) % Y, t),
                ).start()

        for zt, near in ((0, to_low), (Z - 1, to_high)):

            @pl.when(near & (zs != zt))
            def _():
                for_end(zt)

        for j in list(range(1, Y)) + [0]:

            def put_block(at, block):
                if j:
                    yst[zs, j - 1, :, at] = block
                else:
                    rows[t, s, :, at] = block

            picked(zs, z * Y + (y + j) % Y, put_block)
        for j in range(1, Y):
            to = (z * Y + (y + j) % Y, t)
            rcopy(
                yst.at[zs, j - 1], rows.at[t, s], y_s.at[j - 1], rows_r.at[t, s], to
            ).start()
        x_out(s)

    def send_gu(k):
        e = peer(k)
        rcopy(gst.at[k], gub.at[f], gu_s.at[k], gu_r.at[f], (e, t)).start()

    def send_dn(k):
        e = peer(k)
        rcopy(dst.at[k], dnb.at[f], dn_s.at[k], dn_r.at[f], (e, t)).start()

    def come(hop, act_on):
        for zs, there in ((z - hop, z - hop >= 0), (z + hop, z + hop < Z)):
            at = jnp.clip(zs, 0, Z - 1)

            @pl.when(there)
            def _():
                act_on(at)

    def pick_come(at):
        arrived(info.at[at], info_r.at[at])
        pick(at)

    def tok_hop(hop):
        line(tok, by_z, tok_s, tok_r, hop, True)

        @pl.when(inner)
        def _():
            come(hop, pick_come)

    def shared_hop(hop):
        line(shb, by_f, sh_s, sh_r, hop)
        line(sdb, by_f, sd_s, sd_r, hop)
        if hop:
            come(hop, shared_y)
        else:
            shared_y(z)

    pick(z)
    loop(E, convert_gu)
    loop(E, convert_dn)
    gub[f] = gst[E - 1]
    dnb[f] = dst[E - 1]
    if Z > 2:
        tok_hop(1)
    line_sent(tok, by_z, tok_s, 0, True)
    if Z > 2:
        line_sent(tok, by_z, tok_s, 1, True)
    shared_hop(0)
    for hop in range(2, Z - 1):
        tok_hop(hop)
    shared_hop(1)
    line_sent(shb, by_f, sh_s, 0)
    line_sent(sdb, by_f, sd_s, 0)
    loop(half // 2, send_gu)
    loop(E - 1, send_gu, half)

    for i in range(Z):
        zs = jnp.where(z < Z // 2, z + i, z + Z - i) % Z
        for j in range(Y):
            s = zs * Y + (y + j) % Y
            if j:
                arrived(rows.at[t, s], rows_r.at[t, s])
                x_out(s)
            elif i:

                @pl.when(jnp.logical_not(inner))
                def _():
                    arrived(rows.at[t, s], rows_r.at[t, s])
                    x_out(s)

    for hop in range(2, Z - 1):
        shared_hop(hop)
    loop(half // 2, lambda k: sent(gst.at[k], gu_s.at[k]))
    loop(half, send_gu, half // 2)
    for i in range(1, C):
        to_t = (x + i) % C * cores + c

        def forward(s):
            arrived(rows.at[to_t, s], rows_r.at[to_t, s])
            rcopy(
                rows.at[to_t, s], rows.at[to_t, s], part_s.at[i], part_r.at[i],
                (f, x * cores + 1 - c),
            ).start()

        loop(E, forward)
    loop(half, lambda k: sent(gst.at[k], gu_s.at[k]), half // 2)
    loop(E - 1, send_dn)

    def put(src, dst_ref, i):
        copy = pltpu.make_async_copy(src, dst_ref, out_sem.at[i])
        copy.start()
        return copy

    puts = []
    own_cols = pl.ds(pl.multiple_of(t * Dc, Dc), Dc)

    def spread(buf, out, ssem, rsem, i):
        for k in range(1, Pn):
            tt = (t + k) % Pn
            rcopy(
                buf.at[pl.ds(tt * per, per)], out.at[:, :, own_cols], ssem.at[k - 1],
                rsem.at[t], (f, tt),
            ).start()
        return put(buf.at[pl.ds(t * per, per)], out.at[:, :, own_cols], i)

    def spread_wait(buf, out, ssem, rsem):
        for k in range(1, Pn):
            tt = (t + k) % Pn
            sent(buf.at[pl.ds(tt * per, per)], ssem.at[k - 1])
            at = pl.ds(pl.multiple_of(tt * Dc, Dc), Dc)
            arrived(out.at[:, :, at], rsem.at[tt])

    def act(v, width):
        gate, up = v[:, :width], v[:, width:]
        return (gate / (1.0 + jnp.exp(-gate)) * up).astype(BF16)

    mt = min(256, T)

    def shared_in(m):
        at = pl.ds(pl.multiple_of(m * mt, mt), mt)
        total = None
        for q in range(Pn):
            w = shb[q * per : (q + 1) * per].reshape(Dc, 2 * Sc)
            term = jnp.dot(nrm[at, q * Dc : (q + 1) * Dc], w, preferred_element_type=F32)
            total = term if total is None else total + term
        shid[t, at, :] = act(total, Sc)

    def rows_waits():
        part = x * cores + 1 - c
        arrived(rows.at[part], part_r.at[0])
        for i in range(1, C):
            arrived(rows.at[(x + i) % C * cores + 1 - c], part_r.at[i])

    rows_waits()

    def wait_gu(k):
        s = source(k)
        arrived(gub.at[s], gu_r.at[s])

    loop(E - 1, wait_gu)
    puts.append(put(gub.at[:, :, pl.ds(0, Hc)], eg, 4))
    puts.append(put(gub.at[:, :, pl.ds(Hc, Hc)], eu, 5))
    M, g, groups = S.M, S.g, S.groups
    own = f // g

    def group_at(k):
        return ring(k, groups, own) if groups > 1 else 0

    def hidden_in(k):
        q0 = group_at(k)
        span = pl.ds(q0 * g, g)
        total = None
        for q in range(Pn):
            w = gub[q * per : (q + 1) * per].reshape(Dc, 2 * Hc)
            term = jnp.dot(rows[q, span].reshape(M, Dc), w, preferred_element_type=F32)
            total = term if total is None else total + term
        hid[t, span] = act(total, Hc).reshape(g, cap, Hc)

    def send_hidden(k):
        span = pl.ds(group_at(k) * g, g)
        for j in range(1, Pn):
            tt = (t + j) % Pn
            rcopy(
                hid.at[t, span], hid.at[t, span], hid_s.at[j - 1], hid_r.at[t, k], (f, tt)
            ).start()

    def hidden_step(k):
        hidden_in(k)

        @pl.when(k > 0)
        def _():
            send_hidden(k - 1)

    loop(groups, hidden_step)

    def wait_dn(k):
        s = source(k)
        arrived(dnb.at[s], dn_r.at[s])

    send_hidden(groups - 1)
    if Z > 2:
        shared_hop(Z - 1)
    loop(E - 1, wait_dn)
    puts.append(spread(dnb, ed, edo_s, edo_r, 6))

    def send_back(k):
        for i in range(g):
            s = group_at(k) * g + i

            @pl.when(s != f)
            def _():
                rcopy(res.at[s], ret.at[f], ret_s.at[s], ret_r.at[f], (s, t)).start()

    def back_step(k):
        span = pl.ds(group_at(k) * g, g)
        for j in range(1, Pn):
            tt = (t + j) % Pn
            arrived(hid.at[tt, span], hid_r.at[tt, k])

        def part(n):
            at = pl.ds(pl.multiple_of(n * nt, nt), nt)
            total = None
            for q in range(Pn):
                w = dnb[q * per : (q + 1) * per, :, at].reshape(Hc, nt)
                term = jnp.dot(hid[q, span].reshape(M, Hc), w, preferred_element_type=F32)
                total = term if total is None else total + term
            res[span, :, at] = total.astype(BF16).reshape(g, cap, nt)

        loop(Dc // nt, part)
        send_back(k)

    loop(groups, back_step)
    ret[f] = res[f]

    for j in range(1, Y):
        for zs in range(Z):
            s = zs * Y + (y + j) % Y
            arrived(shb.at[s], sh_r.at[s])
            arrived(sdb.at[s], sd_r.at[s])

    puts += [put(shb.at[:, :, pl.ds(0, Sc)], sg, 1), put(shb.at[:, :, pl.ds(Sc, Sc)], su, 2)]
    loop(T // mt, shared_in)

    for k in range(1, Pn):
        rcopy(shid.at[t], shid.at[t], shid_s.at[k - 1], shid_r.at[t], (f, (t + k) % Pn)).start()
    for k in range(1, Pn):
        arrived(shid.at[(t + k) % Pn], shid_r.at[(t + k) % Pn])

    def shared_out(n):
        at = pl.ds(pl.multiple_of(n * nt, nt), nt)
        total = None
        for q in range(Pn):
            w = sdb[q * per : (q + 1) * per, :, at].reshape(Sc, nt)
            term = jnp.dot(shid[q], w, preferred_element_type=F32)
            total = term if total is None else total + term
        acc[:, at] = total

    loop(Dc // nt, shared_out)

    puts.append(spread(sdb, sd, sdo_s, sdo_r, 3))

    routes = route[...].astype(F32)
    named0, named1 = routes[:, 0:1], routes[:, 1:2]
    name_cols = lax.broadcasted_iota(jnp.int32, (T, 128), 1).astype(F32)
    is0, is1 = named0 == name_cols, named1 == name_cols
    chosen_cols = (is0 | is1).astype(F32)
    after = lax.broadcasted_iota(jnp.int32, (T, T), 0) > lax.broadcasted_iota(
        jnp.int32, (T, T), 1
    )
    count_cols = jnp.dot(
        after.astype(F32).astype(BF16), chosen_cols.astype(BF16), preferred_element_type=F32
    )
    target0 = named0 * cap + jnp.sum(jnp.where(is0, count_cols, 0.0), axis=1, keepdims=True)
    target1 = named1 * cap + jnp.sum(jnp.where(is1, count_cols, 0.0), axis=1, keepdims=True)
    w0, w1 = weight[:, 0:1], weight[:, 1:2]

    def combine(i):
        q0 = group_at(groups - 1 - i)
        for j in range(g):
            s = q0 * g + j

            @pl.when(s != f)
            def _():
                arrived(ret.at[s], ret_r.at[s])

        spot = (lax.broadcasted_iota(jnp.int32, (T, M), 1) + q0 * M).astype(F32)
        weigh = jnp.where(target0 == spot, w0, 0.0) + jnp.where(target1 == spot, w1, 0.0)
        weigh = weigh.astype(BF16)

        def part(n):
            at = pl.ds(pl.multiple_of(n * nt, nt), nt)
            block = ret[pl.ds(q0 * g, g), :, at].reshape(M, nt)
            total = acc[:, at] + jnp.dot(weigh, block, preferred_element_type=F32)
            acc[:, at] = total

        loop(Dc // nt, part)

    loop(groups, combine)
    outb[...] = acc[...].astype(BF16)
    puts.append(put(outb, mixed, 7))

    for hop in range(1, Z - 1):
        if hop > 1:
            line_sent(tok, by_z, tok_s, hop, True)
        line_sent(shb, by_f, sh_s, hop)
        line_sent(sdb, by_f, sd_s, hop)
    tell(lambda i, zo: sent(info.at[z], info_s.at[i]))
    for j in range(1, Y):
        sent(shb.at[pl.ds(0, Z)], shy_s.at[j - 1])
        sent(sdb.at[pl.ds(0, Z)], sdy_s.at[j - 1])

        @pl.when(inner)
        def _():
            sent(yst.at[:, j - 1], y_s.at[j - 1])

        @pl.when(jnp.logical_not(inner))
        def _():
            sent(yst.at[0, j - 1], y_s.at[j - 1])

    @pl.when(to_low | to_high)
    def _():
        for j in range(Y):
            sent(est.at[pl.ds(0, Z - 1), j], e_s.at[j])

    for i in range(1, C):
        sent(rows.at[t], x_s.at[i - 1])
    for i in range(C):
        sent(rows.at[t], part_s.at[i])
    loop(E - 1, lambda k: sent(gst.at[k], gu_s.at[k]), half)
    loop(E - 1, lambda k: sent(dst.at[k], dn_s.at[k]))
    for k in range(1, Pn):
        sent(shid.at[t], shid_s.at[k - 1])
        sent(hid.at[t], hid_s.at[k - 1])

    def drain_ret(k):
        s = source(k)
        sent(res.at[s], ret_s.at[s])

    loop(E - 1, drain_ret)
    spread_wait(sdb, sd, sdo_s, sdo_r)
    spread_wait(dnb, ed, edo_s, edo_r)
    for copy in puts:
        copy.wait()


def handed(count, parts, *refs):
    ins, outs, held = refs[:count], refs[count : 2 * count], refs[2 * count : 3 * count]
    in_sem, out_sem = refs[3 * count :]

    def piece(i, j, ref):
        rows = ref.shape[0] // parts
        return ref.at[pl.ds(j * rows, rows)]

    def taken(i, j):
        return pltpu.make_async_copy(piece(i, j, ins[i]), piece(i, j, held[i]), in_sem.at[i, j])

    def given(i, j):
        return pltpu.make_async_copy(piece(i, j, held[i]), piece(i, j, outs[i]), out_sem.at[i, j])

    every = [(i, j) for i in range(count) for j in range(parts)]
    for at in every:
        taken(*at).start()
    for at in every:
        taken(*at).wait()
        given(*at).start()
    for at in every:
        given(*at).wait()


def on_device(
    tokens, norm_gain, gate_train, up_train, down_train,
    shared_gate_train, shared_up_train, shared_down_train, route_expert, route_weight,
):
    S = Sizes(
        lax.axis_size("fs"), lax.axis_size("tp"), tokens.shape, gate_train.shape,
        down_train.shape, shared_gate_train.shape, shared_down_train.shape,
        route_expert.shape[1],
    )
    E, Pn, C, Z, Y = S.E, S.P, S.C, S.Z, S.Y
    T, D, cap, Dr, Hc, Hr, Dc, Sc, Sr, per = (
        S.T, S.D, S.cap, S.Dr, S.Hc, S.Hr, S.Dc, S.Sc, S.Sr, S.per
    )
    dma = pltpu.SemaphoreType.DMA
    anywhere = pl.BlockSpec(memory_space=pl.ANY)
    inside = pl.BlockSpec(memory_space=pltpu.VMEM)
    far = max(1, Y - 1)
    scratch = [
        pltpu.VMEM((T, D), BF16),
        pltpu.VMEM((Z, T, Dc), BF16),
        pltpu.VMEM((Z, 8, T), F32),
        pltpu.VMEM((E, Dr, 2 * Sc), BF16),
        pltpu.VMEM((E, Sr, Dc), BF16),
        pltpu.VMEM((E, Dr, 2 * Hc), BF16),
        pltpu.VMEM((E, Dr, 2 * Hc), BF16),
        pltpu.VMEM((E, Hr, Dc), BF16),
        pltpu.VMEM((E, Hr, Dc), BF16),
        pltpu.VMEM((Pn, E, cap, Dc), BF16),
        pltpu.VMEM((Z, far, cap, Dc), BF16),
        pltpu.VMEM((Z, Y, cap, Dc), BF16),
        pltpu.VMEM((Pn, E, cap, Hc), BF16),
        pltpu.VMEM((E, cap, Dc), BF16),
        pltpu.VMEM((E, cap, Dc), BF16),
        pltpu.VMEM((T, Dc), F32),
        pltpu.VMEM((Pn, T, Sc), BF16),
        pltpu.VMEM((T, Dc), BF16),
        pltpu.VMEM((2, 2, Dr, Hc), F32),
        pltpu.VMEM((2, Hr, Dc), F32),
        pltpu.VMEM((Dr, 128), F32),
        dma((2, 3)), dma((1,)), dma((8,)),
        dma((2, Z)), dma((Z,)), dma((Z,)), dma((Z,)),
        dma((2, Z)), dma((E,)), dma((far,)),
        dma((2, Z)), dma((E,)), dma((far,)),
        dma((E,)), dma((E,)), dma((E,)), dma((E,)),
        dma((far,)), dma((Y,)), dma((Pn, E)), dma((C,)), dma((C,)), dma((C,)),
        dma((Pn,)), dma((Pn, S.groups)), dma((Pn,)), dma((Pn,)),
        dma((Pn,)), dma((Pn,)), dma((Pn,)), dma((Pn,)),
        dma((E,)), dma((E,)),
    ]
    shape = lambda *dims: jax.ShapeDtypeStruct(dims, BF16)
    flops = 2 * T * D * 2 * Sc + 2 * E * cap * D * 2 * Hc + 4 * E * cap * D * Hc
    outs = pl.pallas_call(
        functools.partial(kernel, S),
        out_shape=[
            shape(E, Dr, Hc), shape(E, Dr, Hc), shape(per, Hr, D),
            shape(E, Dr, Sc), shape(E, Dr, Sc), shape(per, Sr, D), shape(T, Dc),
        ],
        in_specs=[anywhere] * 7 + [inside] * 3,
        out_specs=[anywhere] * 7,
        scratch_shapes=scratch,
        compiler_params=pltpu.CompilerParams(
            collective_id=0, has_side_effects=True, vmem_limit_bytes=67043328
        ),
        cost_estimate=pl.CostEstimate(flops=flops, bytes_accessed=1 << 26, transcendentals=0),
    )(
        tokens, gate_train, up_train, down_train, shared_gate_train, shared_up_train,
        shared_down_train, norm_gain[None, :], route_expert, route_weight,
    )
    parts = 2
    in_hbm = pl.BlockSpec(memory_space=pl.ANY)
    eg, eu, ed, sg, su, sd, mixed = pl.pallas_call(
        functools.partial(handed, len(outs), parts),
        out_shape=[jax.ShapeDtypeStruct(o.shape, o.dtype) for o in outs],
        in_specs=[in_hbm] * len(outs),
        out_specs=[in_hbm] * len(outs),
        scratch_shapes=[pltpu.VMEM(o.shape, o.dtype) for o in outs]
        + [dma((len(outs), parts))] * 2,
        compiler_params=pltpu.CompilerParams(vmem_limit_bytes=62 << 20),
    )(*outs)
    return (
        eg.reshape(1, D, Hc), eu.reshape(1, D, Hc), ed.reshape(1, per * Hr, D),
        sg.reshape(D, Sc), su.reshape(D, Sc), sd.reshape(per * Sr, D), mixed,
    )


def solution(mesh):
    placed = (
        P("fs", None),
        P("fs"),
        P(None, "fs", "tp"),
        P(None, "fs", "tp"),
        P(None, "fs", "tp"),
        P("fs", "tp"),
        P("fs", "tp"),
        P("fs", "tp"),
        P("fs", None),
        P("fs", None),
    )
    return jax.shard_map(
        on_device,
        mesh=mesh,
        in_specs=placed,
        out_specs=(
            P("fs", None, "tp"),
            P("fs", None, "tp"),
            P("fs", "tp", None),
            P(None, "tp"),
            P(None, "tp"),
            P("tp", None),
            P("fs", "tp"),
        ),
        check_vma=False,
    )
```

```python
import functools

import jax
import jax.numpy as jnp
from jax import lax
from jax.experimental import pallas as pl
from jax.experimental.pallas import tpu as pltpu
from jax.sharding import PartitionSpec as P

norm_eps = 1e-06
cores = 2
MESH = pl.DeviceIdType.MESH
F32, BF16 = jnp.float32, jnp.bfloat16


class Sizes:
    def __init__(self, experts, pieces, tokens, gate, down, sgate, sdown, top):
        self.E, self.P = experts, pieces
        self.C = pieces // cores
        long = 1
        while long * long < experts:
            long *= 2
        self.Z, self.Y = long, experts // long
        self.half = experts // 2
        self.T, self.D = tokens
        self.cap = 3 * self.T * top // (2 * experts)
        self.Dr, self.Hc = gate[1:]
        self.Hr, self.Dc = down[1:]
        self.Dr2, self.Sc = sgate
        self.Sr = sdown[0]
        self.per = experts // pieces
        self.g = 1
        while self.g * self.cap % 128:
            self.g *= 2
        self.groups = experts // self.g
        self.M = self.g * self.cap
        self.nt = min(256, self.Dc)


def kernel(
    S,
    tokens, gate_t, up_t, down_t, sgate_t, sup_t, sdown_t, gain, route, weight,
    eg, eu, ed, sg, su, sd, mixed,
    nrm, tok, info, shb, sdb, gst, gub, dst, dnb, rows, yst, est, hid, res, ret, cmb, farin, acc, shid, outb,
    wbuf, dbuf, gcol,
    ld_sem, tk_ld, out_sem,
    tok_s, tok_r, info_s, info_r, sh_s, sh_r, shy_s, sd_s, sd_r, sdy_s,
    gu_s, gu_r, dn_s, dn_r, y_s, e_s, rows_r, x_s, part_s, part_r,
    hid_s, hid_r, shid_s, shid_r, edo_s, edo_r, sdo_s, sdo_r, ret_s, ret_r,
    cmb_r, far_s, far_r,
):
    E, Pn, C, Z, Y, half, per = S.E, S.P, S.C, S.Z, S.Y, S.half, S.per
    cap, Dc, Hc, Sc, nt = S.cap, S.Dc, S.Hc, S.Sc, S.nt
    f, t = lax.axis_index("fs"), lax.axis_index("tp")
    z, y = f // Y, f % Y
    x, c = t // cores, t % cores
    inner = (z > 0) & (z < Z - 1)
    to_low, to_high = z == 1, z == Z - 2

    def peer(k):
        span = Z // 2
        p = k // Y
        near = p // span
        plane = (z // span + 1 + near) % 2 * span + (z + p + near) % span
        return plane * Y + (y + 1 + k % Y) % Y

    def rcopy(src, dst, ssem, rsem, to):
        return pltpu.make_async_remote_copy(
            src_ref=src, dst_ref=dst, send_sem=ssem, recv_sem=rsem,
            device_id=to, device_id_type=MESH,
        )

    def arrived(ref, rsem):
        rcopy(ref, ref, out_sem.at[0], rsem, ((f + 1) % E, t)).wait_recv()

    def sent(ref, ssem):
        rcopy(ref, ref, ssem, out_sem.at[0], ((f + 1) % E, t)).wait_send()

    def loop(count, body, start=0):
        lax.fori_loop(start, count, lambda i, v: (body(i), v)[1], 0)

    def load_w(k, slot):
        e = peer(k)
        return [
            pltpu.make_async_copy(w.at[e], wbuf.at[slot, i], ld_sem.at[slot, i])
            for i, w in ((0, gate_t), (1, up_t))
        ]

    def load_d(k, slot):
        return pltpu.make_async_copy(down_t.at[peer(k)], dbuf.at[slot], ld_sem.at[slot, 2])

    tok_load = pltpu.make_async_copy(tokens, nrm, tk_ld.at[0])
    tok_load.start()
    sh_loads = [
        pltpu.make_async_copy(sgate_t, wbuf.at[1, 0], ld_sem.at[1, 0]),
        pltpu.make_async_copy(sup_t, wbuf.at[1, 1], ld_sem.at[1, 1]),
        pltpu.make_async_copy(sdown_t, dbuf.at[1], ld_sem.at[1, 2]),
    ]
    for copy in sh_loads + load_w(0, 0) + [load_d(0, 0)]:
        copy.start()
    greet = pltpu.get_barrier_semaphore()
    for i in range(1, E):
        pl.semaphore_signal(greet, inc=1, device_id=((f + i) % E, t), device_id_type=MESH)
    for i in range(1, Pn):
        pl.semaphore_signal(greet, inc=1, device_id=(f, (t + i) % Pn), device_id_type=MESH)

    T = S.T
    gcol[...] = jnp.broadcast_to(gain[...], (128, S.Dr)).T
    for copy in sh_loads:
        copy.wait()
    shb[f, :, 0:Sc] = (gcol[:, 0:1] * wbuf[1, 0]).astype(BF16)
    shb[f, :, Sc:] = (gcol[:, 0:1] * wbuf[1, 1]).astype(BF16)
    sdb[f] = dbuf[1].astype(BF16)

    by_z = lambda zs: zs
    by_f = lambda zs: zs * Y + y

    def lanes_of(slot_of, hop, within):
        low, high = (1, Z - 1) if within else (0, Z)
        for d in range(2):
            zs = z - hop if d == 0 else z + hop
            there = (zs >= 0) if d == 0 else (zs < Z)
            if within and hop:
                there &= inner
            onward = (z + 1 < high) if d == 0 else (z > low)
            yield d, there, onward, slot_of(jnp.clip(zs, 0, Z - 1)), f + Y if d == 0 else f - Y

    def line(buf, slot_of, ssem, rsem, hop, within=False):
        for d, there, onward, slot, nxt in lanes_of(slot_of, hop, within):

            @pl.when(there)
            def _():
                if hop:
                    arrived(buf.at[slot], rsem.at[slot])

                @pl.when(onward)
                def _():
                    rcopy(
                        buf.at[slot], buf.at[slot], ssem.at[d, hop], rsem.at[slot], (nxt, t)
                    ).start()

    def line_sent(buf, slot_of, ssem, hop, within=False):
        for d, there, onward, slot, nxt in lanes_of(slot_of, hop, within):

            @pl.when(there & onward)
            def _():
                sent(buf.at[slot], ssem.at[d, hop])


    def shared_y(zs):
        s = by_f(zs)
        for j in range(1, Y):
            to = (z * Y + (y + j) % Y, t)
            rcopy(shb.at[s], shb.at[s], shy_s.at[j - 1], sh_r.at[s], to).start()
            rcopy(sdb.at[s], sdb.at[s], sdy_s.at[j - 1], sd_r.at[s], to).start()

    def come(hop, act_on):
        for zs, there in ((z - hop, z - hop >= 0), (z + hop, z + hop < Z)):
            at = jnp.clip(zs, 0, Z - 1)

            @pl.when(there)
            def _():
                act_on(at)

    def shared_hop(hop):
        line(shb, by_f, sh_s, sh_r, hop)
        line(sdb, by_f, sd_s, sd_r, hop)
        if hop:
            come(hop, shared_y)
        else:
            shared_y(z)

    pl.semaphore_wait(greet, E + Pn - 2)
    shared_hop(0)
    wide = max(16, E)
    r0, r1 = route[0:1, :].astype(F32), route[1:2, :].astype(F32)
    names = lax.broadcasted_iota(jnp.int32, (wide, T), 0).astype(F32)
    hit0, hit1 = r0 == names, r1 == names
    chosen = (hit0 | hit1).astype(F32).astype(BF16)
    before = lax.broadcasted_iota(jnp.int32, (T, T), 0) < lax.broadcasted_iota(
        jnp.int32, (T, T), 1
    )
    count = jnp.dot(chosen, before.astype(F32).astype(BF16), preferred_element_type=F32)
    s0 = jnp.sum(jnp.where(hit0, count, 0.0), axis=0, keepdims=True)
    s1 = jnp.sum(jnp.where(hit1, count, 0.0), axis=0, keepdims=True)
    info[z, 0:1, :] = r0
    info[z, 1:2, :] = r1
    info[z, 2:3, :] = s0
    info[z, 3:4, :] = s1
    info[z, 4:6, :] = weight[...]

    tok_load.wait()
    tile = min(64, T)

    def normalise(i):
        at = pl.ds(pl.multiple_of(i * tile, tile), tile)
        v = nrm[at, :].astype(F32)
        v = v * lax.rsqrt(jnp.mean(v * v, axis=1, keepdims=True) + norm_eps)
        nrm[at, :] = v.astype(BF16)
        tok[z, at, :] = nrm[at, pl.ds(pl.multiple_of(t * Dc, Dc), Dc)]

    loop(T // tile, normalise)

    def tell(act_on):
        for i in range(1, Z):
            zo = (z + i) % Z

            @pl.when((zo > 0) & (zo < Z - 1))
            def _():
                act_on(i - 1, zo)

    tell(
        lambda i, zo: rcopy(
            info.at[z], info.at[z], info_s.at[i], info_r.at[z], (zo * Y + y, t)
        ).start()
    )
    line(tok, by_z, tok_s, tok_r, 0, True)

    def convert_gu(k):
        slot = k % 2
        for copy in load_w(k, slot):
            copy.wait()

        @pl.when(k + 1 < E)
        def _():
            for copy in load_w(k + 1, 1 - slot):
                copy.start()

        for i in range(2):
            gst[k, :, i * Hc : (i + 1) * Hc] = (gcol[:, 0:1] * wbuf[slot, i]).astype(BF16)

    def convert_dn(k):
        slot = k % 2
        load_d(k, slot).wait()

        @pl.when(k + 1 < E)
        def _():
            load_d(k + 1, 1 - slot).start()

        dst[k] = dbuf[slot].astype(BF16)

    def x_out(s):
        for i in range(1, C):
            to = (f, (x + i) % C * cores + c)
            rcopy(rows.at[t, s], rows.at[t, s], x_s.at[i - 1], rows_r.at[t, s], to).start()
        rcopy(rows.at[t, s], rows.at[t, s], part_s.at[0], part_r.at[0], (f, x * cores + 1 - c)).start()

    def picked(zs, e, put_block):
        e = e.astype(F32)
        slots = lax.broadcasted_iota(jnp.int32, (cap, T), 0).astype(F32)
        got = (info[zs, 0:1, :] == e) & (info[zs, 2:3, :] == slots)
        got |= (info[zs, 1:2, :] == e) & (info[zs, 3:4, :] == slots)
        got = got.astype(F32).astype(BF16)

        def part(n):
            at = pl.ds(pl.multiple_of(n * nt, nt), nt)
            put_block(at, jnp.dot(got, tok[zs, :, at], preferred_element_type=F32).astype(BF16))

        loop(Dc // nt, part)

    def pick(zs):
        s = by_f(zs)

        def for_end(zt):
            for j in range(Y):

                def put_block(at, block):
                    est[zs, j, :, at] = block

                picked(zs, zt * Y + (y + j) % Y, put_block)
            for j in range(Y):
                rcopy(
                    est.at[zs, j], rows.at[t, s], e_s.at[j], rows_r.at[t, s],
                    (zt * Y + (y + j) % Y, t),
                ).start()

        for zt, near in ((0, to_low), (Z - 1, to_high)):

            @pl.when(near & (zs != zt))
            def _():
                for_end(zt)

        for j in list(range(1, Y)) + [0]:

            def put_block(at, block):
                if j:
                    yst[zs, j - 1, :, at] = block
                else:
                    rows[t, s, :, at] = block

            picked(zs, z * Y + (y + j) % Y, put_block)
        for j in range(1, Y):
            to = (z * Y + (y + j) % Y, t)
            rcopy(
                yst.at[zs, j - 1], rows.at[t, s], y_s.at[j - 1], rows_r.at[t, s], to
            ).start()
        x_out(s)

    def send_gu(k):
        e = peer(k)
        rcopy(gst.at[k], gub.at[f], gu_s.at[k], gu_r.at[f], (e, t)).start()

    def send_dn(k):
        e = peer(k)
        rcopy(dst.at[k], dnb.at[f], dn_s.at[k], dn_r.at[f], (e, t)).start()

    def pick_come(at):
        arrived(info.at[at], info_r.at[at])
        pick(at)

    def tok_hop(hop):
        line(tok, by_z, tok_s, tok_r, hop, True)

        @pl.when(inner)
        def _():
            come(hop, pick_come)

    pick(z)
    loop(E, convert_gu)
    loop(E, convert_dn)
    gub[f] = gst[E - 1]
    dnb[f] = dst[E - 1]
    for hop in range(1, Z - 1):
        tok_hop(hop)
        shared_hop(hop)
        line_sent(tok, by_z, tok_s, hop - 1, True)
        line_sent(shb, by_f, sh_s, hop - 1)
        line_sent(sdb, by_f, sd_s, hop - 1)
    if Z == 2:
        line_sent(tok, by_z, tok_s, 0, True)
        line_sent(shb, by_f, sh_s, 0)
        line_sent(sdb, by_f, sd_s, 0)
    if Z > 2:
        line_sent(tok, by_z, tok_s, Z - 2, True)
    loop(half // 2, send_gu)
    loop(E - 1, send_gu, half)

    for i in range(Z):
        zs = jnp.where(z < Z // 2, z + i, z + Z - i) % Z
        for j in range(Y):
            s = zs * Y + (y + j) % Y
            if j:
                arrived(rows.at[t, s], rows_r.at[t, s])
                x_out(s)
            elif i:

                @pl.when(jnp.logical_not(inner))
                def _():
                    arrived(rows.at[t, s], rows_r.at[t, s])
                    x_out(s)

    loop(half // 2, lambda k: sent(gst.at[k], gu_s.at[k]))
    loop(half, send_gu, half // 2)
    loop(E - 1, send_dn, half)
    for i in range(1, C):
        to_t = (x + i) % C * cores + c

        def forward(s):
            arrived(rows.at[to_t, s], rows_r.at[to_t, s])
            rcopy(
                rows.at[to_t, s], rows.at[to_t, s], part_s.at[i], part_r.at[i],
                (f, x * cores + 1 - c),
            ).start()

        loop(E, forward)
    def put(src, dst_ref, i):
        copy = pltpu.make_async_copy(src, dst_ref, out_sem.at[i])
        copy.start()
        return copy

    puts = []
    own_cols = pl.ds(pl.multiple_of(t * Dc, Dc), Dc)

    def spread(buf, out, ssem, rsem, i):
        for k in range(1, Pn):
            tt = (t + k) % Pn
            rcopy(
                buf.at[pl.ds(tt * per, per)], out.at[:, :, own_cols], ssem.at[k - 1],
                rsem.at[t], (f, tt),
            ).start()
        return put(buf.at[pl.ds(t * per, per)], out.at[:, :, own_cols], i)

    def spread_wait(buf, out, ssem, rsem):
        for k in range(1, Pn):
            tt = (t + k) % Pn
            sent(buf.at[pl.ds(tt * per, per)], ssem.at[k - 1])
            at = pl.ds(pl.multiple_of(tt * Dc, Dc), Dc)
            arrived(out.at[:, :, at], rsem.at[tt])

    if Z > 2:
        shared_hop(Z - 1)
    loop(half, lambda k: sent(gst.at[k], gu_s.at[k]), half // 2)

    def act(v, width):
        gate, up = v[:, :width], v[:, width:]
        return (gate / (1.0 + jnp.exp(-gate)) * up).astype(BF16)

    mt = min(256, T)

    def shared_in(m):
        at = pl.ds(pl.multiple_of(m * mt, mt), mt)
        total = None
        for q in range(Pn):
            w = shb[q * per : (q + 1) * per].reshape(Dc, 2 * Sc)
            term = jnp.dot(nrm[at, q * Dc : (q + 1) * Dc], w, preferred_element_type=F32)
            total = term if total is None else total + term
        shid[t, at, :] = act(total, Sc)

    def inner_of(s):
        return (s // Y > 0) & (s // Y < Z - 1)

    def rows_waits():
        part = x * cores + 1 - c
        arrived(rows.at[part], part_r.at[0])
        for i in range(1, C):
            arrived(rows.at[(x + i) % C * cores + 1 - c], part_r.at[i])

    rows_waits()

    def wait_gu(k):
        s = peer(k)
        arrived(gub.at[s], gu_r.at[s])

    loop(E - 1, wait_gu)
    loop(half, send_dn)
    puts.append(put(gub.at[:, :, pl.ds(0, Hc)], eg, 4))
    puts.append(put(gub.at[:, :, pl.ds(Hc, Hc)], eu, 5))
    M, g, groups = S.M, S.g, S.groups
    own = f // g

    low = f < half
    side = groups // 2
    mid_z = jnp.where(low, Z // 2 - 1, Z // 2)
    over_z = jnp.where(low, Z // 2, Z // 2 - 1)

    def group_at(k):
        far = jnp.where(low, groups - 1 - k, k)
        near = own // side * side + (own + 1 + k - side) % side
        return jnp.where(k < side, far, near)

    def hidden_in(k):
        q0 = group_at(k)
        span = pl.ds(q0 * g, g)
        total = None
        for q in range(Pn):
            w = gub[q * per : (q + 1) * per].reshape(Dc, 2 * Hc)
            term = jnp.dot(rows[q, span].reshape(M, Dc), w, preferred_element_type=F32)
            total = term if total is None else total + term
        hid[t, span] = act(total, Hc).reshape(g, cap, Hc)

    partner = x * cores + 1 - c

    def pass_hidden(i, tt, k, to):
        span = pl.ds(group_at(k) * g, g)
        rcopy(hid.at[tt, span], hid.at[tt, span], hid_s.at[i], hid_r.at[tt, k], (f, to)).start()

    def send_hidden(k):
        for i in range(1, C):
            pass_hidden(i, t, k, (x + i) % C * cores + c)
        pass_hidden(0, t, k, partner)

    def forward_hidden(k):
        span = pl.ds(group_at(k) * g, g)
        for i in range(1, C):
            tt = (x + i) % C * cores + c
            arrived(hid.at[tt, span], hid_r.at[tt, k])
            pass_hidden(C - 1 + i, tt, k, partner)

    def hidden_step(k):
        hidden_in(k)

        @pl.when(k > 0)
        def _():
            send_hidden(k - 1)

    loop(groups, hidden_step)

    def wait_dn(k):
        s = peer(k)
        arrived(dnb.at[s], dn_r.at[s])

    send_hidden(groups - 1)
    for j in range(1, Y):
        for zs in range(Z):
            s = zs * Y + (y + j) % Y
            arrived(shb.at[s], sh_r.at[s])
            arrived(sdb.at[s], sd_r.at[s])

    puts += [put(shb.at[:, :, pl.ds(0, Sc)], sg, 1), put(shb.at[:, :, pl.ds(Sc, Sc)], su, 2)]
    loop(T // mt, shared_in)

    for k in range(1, Pn):
        rcopy(shid.at[t], shid.at[t], shid_s.at[k - 1], shid_r.at[t], (f, (t + k) % Pn)).start()
    puts.append(spread(sdb, sd, sdo_s, sdo_r, 3))
    loop(groups, forward_hidden)
    loop(E - 1, wait_dn)

    def send_back(k):
        for i in range(g):
            s = group_at(k) * g + i
            over = (s // Y == over_z) & inner_of(s)
            to = mid_z * Y + s % Y

            @pl.when(over & (to != f))
            def _():
                rcopy(res.at[s], cmb.at[f % half], ret_s.at[s], cmb_r.at[f % half], (to, t)).start()

            @pl.when(jnp.logical_not(over) & (s != f))
            def _():
                rcopy(res.at[s], ret.at[f], ret_s.at[s], ret_r.at[f], (s, t)).start()

    def back_step(k):
        span = pl.ds(group_at(k) * g, g)

        for i in range(C):
            tt = (x + i) % C * cores + 1 - c
            arrived(hid.at[tt, span], hid_r.at[tt, k])

        def part(n):
            at = pl.ds(pl.multiple_of(n * nt, nt), nt)
            total = None
            for q in range(Pn):
                w = dnb[q * per : (q + 1) * per, :, at].reshape(Hc, nt)
                term = jnp.dot(hid[q, span].reshape(M, Hc), w, preferred_element_type=F32)
                total = term if total is None else total + term
            res[span, :, at] = total.astype(BF16).reshape(g, cap, nt)

        loop(Dc // nt, part)
        send_back(k)

    loop(groups, back_step)
    ret[f] = res[f]

    def weigh(zs, base, many):
        spot = (lax.broadcasted_iota(jnp.int32, (many, T), 0) + base).astype(F32)
        at0 = info[zs, 0:1, :] * cap + info[zs, 2:3, :]
        at1 = info[zs, 1:2, :] * cap + info[zs, 3:4, :]
        share = jnp.where(at0 == spot, info[zs, 4:5, :], 0.0)
        share += jnp.where(at1 == spot, info[zs, 5:6, :], 0.0)
        return share.T.astype(BF16)

    puts.append(spread(dnb, ed, edo_s, edo_r, 6))
    @pl.when(inner)
    def _():
        to = over_z * Y + y
        cmb[f % half] = res[to]
        for i in range(1, half):
            e = (f + i) % half
            arrived(cmb.at[e], cmb_r.at[e])
        many = half * cap
        shares = weigh(over_z, f // half * many, many)

        def part(n):
            at = pl.ds(pl.multiple_of(n * nt, nt), nt)
            block = cmb[:, :, at].reshape(many, nt)
            tok[0, :, at] = jnp.dot(shares, block, preferred_element_type=F32).astype(BF16)

        loop(Dc // nt, part)
        rcopy(tok.at[0], farin, far_s.at[0], far_r.at[0], (to, t)).start()


    for k in range(1, Pn):
        arrived(shid.at[(t + k) % Pn], shid_r.at[(t + k) % Pn])

    def shared_out(n):
        at = pl.ds(pl.multiple_of(n * nt, nt), nt)
        total = None
        for q in range(Pn):
            w = sdb[q * per : (q + 1) * per, :, at].reshape(Sc, nt)
            term = jnp.dot(shid[q], w, preferred_element_type=F32)
            total = term if total is None else total + term
        acc[:, at] = total

    loop(Dc // nt, shared_out)


    def combine(k):
        q0 = group_at(groups - 1 - k)
        for j in range(g):
            s = q0 * g + j

            @pl.when(s != f)
            def _():
                arrived(ret.at[s], ret_r.at[s])

        shares = weigh(z, q0 * M, M)

        def part(n):
            at = pl.ds(pl.multiple_of(n * nt, nt), nt)
            block = ret[pl.ds(q0 * g, g), :, at].reshape(M, nt)
            acc[:, at] += jnp.dot(shares, block, preferred_element_type=F32)

        loop(Dc // nt, part)

    loop(side, combine)

    @pl.when(jnp.logical_not(inner))
    def _():
        loop(groups, combine, side)

    @pl.when(inner)
    def _():
        arrived(farin, far_r.at[0])
        acc[...] += farin[...].astype(F32)

    outb[...] = acc[...].astype(BF16)
    puts.append(put(outb, mixed, 7))

    if Z > 2:
        line_sent(shb, by_f, sh_s, Z - 2)
        line_sent(sdb, by_f, sd_s, Z - 2)
    tell(lambda i, zo: sent(info.at[z], info_s.at[i]))
    for j in range(1, Y):
        sent(shb.at[pl.ds(0, Z)], shy_s.at[j - 1])
        sent(sdb.at[pl.ds(0, Z)], sdy_s.at[j - 1])

        @pl.when(inner)
        def _():
            sent(yst.at[:, j - 1], y_s.at[j - 1])

        @pl.when(jnp.logical_not(inner))
        def _():
            sent(yst.at[0, j - 1], y_s.at[j - 1])

    @pl.when(to_low | to_high)
    def _():
        for j in range(Y):
            sent(est.at[pl.ds(0, Z - 1), j], e_s.at[j])

    for i in range(1, C):
        sent(rows.at[t], x_s.at[i - 1])
    for i in range(C):
        sent(rows.at[t], part_s.at[i])
    loop(E - 1, lambda k: sent(gst.at[k], gu_s.at[k]), half)
    loop(E - 1, lambda k: sent(dst.at[k], dn_s.at[k]))
    for k in range(1, Pn):
        sent(shid.at[t], shid_s.at[k - 1])
        sent(hid.at[t], hid_s.at[k - 1])

    def drain_ret(k):
        s = peer(k)

        @pl.when(jnp.logical_not(inner & (s == over_z * Y + y)))
        def _():
            sent(res.at[s], ret_s.at[s])

    @pl.when(inner)
    def _():
        sent(tok.at[0], far_s.at[0])

    loop(E - 1, drain_ret)
    spread_wait(sdb, sd, sdo_s, sdo_r)
    spread_wait(dnb, ed, edo_s, edo_r)
    for copy in puts:
        copy.wait()


def handed(count, parts, *refs):
    ins, outs, held = refs[:count], refs[count : 2 * count], refs[2 * count : 3 * count]
    in_sem, out_sem = refs[3 * count :]

    def piece(i, j, ref):
        rows = ref.shape[0] // parts
        return ref.at[pl.ds(j * rows, rows)]

    def taken(i, j):
        return pltpu.make_async_copy(piece(i, j, ins[i]), piece(i, j, held[i]), in_sem.at[i, j])

    def given(i, j):
        return pltpu.make_async_copy(piece(i, j, held[i]), piece(i, j, outs[i]), out_sem.at[i, j])

    every = [(i, j) for i in range(count) for j in range(parts)]
    for at in every:
        taken(*at).start()
    for at in every:
        taken(*at).wait()
        given(*at).start()
    for at in every:
        given(*at).wait()


def on_device(
    tokens, norm_gain, gate_train, up_train, down_train,
    shared_gate_train, shared_up_train, shared_down_train, route_expert, route_weight,
):
    S = Sizes(
        lax.axis_size("fs"), lax.axis_size("tp"), tokens.shape, gate_train.shape,
        down_train.shape, shared_gate_train.shape, shared_down_train.shape,
        route_expert.shape[1],
    )
    E, Pn, C, Z, Y = S.E, S.P, S.C, S.Z, S.Y
    T, D, cap, Dr, Hc, Hr, Dc, Sc, Sr, per = (
        S.T, S.D, S.cap, S.Dr, S.Hc, S.Hr, S.Dc, S.Sc, S.Sr, S.per
    )
    dma = pltpu.SemaphoreType.DMA
    anywhere = pl.BlockSpec(memory_space=pl.ANY)
    inside = pl.BlockSpec(memory_space=pltpu.VMEM)
    far = max(1, Y - 1)
    scratch = [
        pltpu.VMEM((T, D), BF16),
        pltpu.VMEM((Z, T, Dc), BF16),
        pltpu.VMEM((Z, 8, T), F32),
        pltpu.VMEM((E, Dr, 2 * Sc), BF16),
        pltpu.VMEM((E, Sr, Dc), BF16),
        pltpu.VMEM((E, Dr, 2 * Hc), BF16),
        pltpu.VMEM((E, Dr, 2 * Hc), BF16),
        pltpu.VMEM((E, Hr, Dc), BF16),
        pltpu.VMEM((E, Hr, Dc), BF16),
        pltpu.VMEM((Pn, E, cap, Dc), BF16),
        pltpu.VMEM((Z, far, cap, Dc), BF16),
        pltpu.VMEM((Z, Y, cap, Dc), BF16),
        pltpu.VMEM((Pn, E, cap, Hc), BF16),
        pltpu.VMEM((E, cap, Dc), BF16),
        pltpu.VMEM((E, cap, Dc), BF16),
        pltpu.VMEM((E // 2, cap, Dc), BF16),
        pltpu.VMEM((T, Dc), BF16),
        pltpu.VMEM((T, Dc), F32),
        pltpu.VMEM((Pn, T, Sc), BF16),
        pltpu.VMEM((T, Dc), BF16),
        pltpu.VMEM((2, 2, Dr, Hc), F32),
        pltpu.VMEM((2, Hr, Dc), F32),
        pltpu.VMEM((Dr, 128), F32),
        dma((2, 3)), dma((1,)), dma((8,)),
        dma((2, Z)), dma((Z,)), dma((Z,)), dma((Z,)),
        dma((2, Z)), dma((E,)), dma((far,)),
        dma((2, Z)), dma((E,)), dma((far,)),
        dma((E,)), dma((E,)), dma((E,)), dma((E,)),
        dma((far,)), dma((Y,)), dma((Pn, E)), dma((C,)), dma((C,)), dma((C,)),
        dma((Pn,)), dma((Pn, S.groups)), dma((Pn,)), dma((Pn,)),
        dma((Pn,)), dma((Pn,)), dma((Pn,)), dma((Pn,)),
        dma((E,)), dma((E,)),
        dma((E // 2,)), dma((1,)), dma((1,)),
    ]
    shape = lambda *dims: jax.ShapeDtypeStruct(dims, BF16)
    flops = 2 * T * D * 2 * Sc + 2 * E * cap * D * 2 * Hc + 4 * E * cap * D * Hc
    outs = pl.pallas_call(
        functools.partial(kernel, S),
        out_shape=[
            shape(E, Dr, Hc), shape(E, Dr, Hc), shape(per, Hr, D),
            shape(E, Dr, Sc), shape(E, Dr, Sc), shape(per, Sr, D), shape(T, Dc),
        ],
        in_specs=[anywhere] * 7 + [inside] * 3,
        out_specs=[anywhere] * 7,
        scratch_shapes=scratch,
        compiler_params=pltpu.CompilerParams(
            collective_id=0, has_side_effects=True, vmem_limit_bytes=67043328
        ),
        cost_estimate=pl.CostEstimate(flops=flops, bytes_accessed=1 << 26, transcendentals=0),
    )(
        tokens, gate_train, up_train, down_train, shared_gate_train, shared_up_train,
        shared_down_train, norm_gain[None, :], route_expert.T, route_weight.T,
    )
    parts = 2
    in_hbm = pl.BlockSpec(memory_space=pl.ANY)
    eg, eu, ed, sg, su, sd, mixed = pl.pallas_call(
        functools.partial(handed, len(outs), parts),
        out_shape=[jax.ShapeDtypeStruct(o.shape, o.dtype) for o in outs],
        in_specs=[in_hbm] * len(outs),
        out_specs=[in_hbm] * len(outs),
        scratch_shapes=[pltpu.VMEM(o.shape, o.dtype) for o in outs]
        + [dma((len(outs), parts))] * 2,
        compiler_params=pltpu.CompilerParams(vmem_limit_bytes=62 << 20),
    )(*outs)
    return (
        eg.reshape(1, D, Hc), eu.reshape(1, D, Hc), ed.reshape(1, per * Hr, D),
        sg.reshape(D, Sc), su.reshape(D, Sc), sd.reshape(per * Sr, D), mixed,
    )


def solution(mesh):
    placed = (
        P("fs", None),
        P("fs"),
        P(None, "fs", "tp"),
        P(None, "fs", "tp"),
        P(None, "fs", "tp"),
        P("fs", "tp"),
        P("fs", "tp"),
        P("fs", "tp"),
        P("fs", None),
        P("fs", None),
    )
    return jax.shard_map(
        on_device,
        mesh=mesh,
        in_specs=placed,
        out_specs=(
            P("fs", None, "tp"),
            P("fs", None, "tp"),
            P("fs", "tp", None),
            P(None, "tp"),
            P(None, "tp"),
            P("tp", None),
            P("fs", "tp"),
        ),
        check_vma=False,
    )
```

```python
import functools
import math

import jax
import jax.numpy as jnp
from jax import lax
from jax.experimental import pallas as pl
from jax.experimental.pallas import tpu as pltpu
from jax.sharding import PartitionSpec as P

norm_eps = 1e-06
cores = 2
MESH = pl.DeviceIdType.MESH
F32, BF16 = jnp.float32, jnp.bfloat16


class Sizes:
    def __init__(self, experts, pieces, tokens, gate, down, sgate, sdown, top):
        self.E, self.P = experts, pieces
        self.C = pieces // cores
        long = 1
        while long * long < experts:
            long *= 2
        self.Z, self.Y = long, experts // long
        self.half = experts // 2
        self.T, self.D = tokens
        self.cap = 3 * self.T * top // (2 * experts)
        self.Dr, self.Hc = gate[1:]
        self.Hr, self.Dc = down[1:]
        self.Dr2, self.Sc = sgate
        self.Sr = sdown[0]
        self.per = experts // pieces
        self.g = 1
        while self.g * self.cap % 128:
            self.g *= 2
        self.groups = experts // self.g
        self.M = self.g * self.cap
        self.nt = min(256, self.Dc)
        assert self.groups <= self.Z and self.M <= self.T


def kernel(
    S,
    tokens, gate_t, up_t, down_t, sgate_t, sup_t, sdown_t, gain, route, weight,
    gub, shb, outb, ed, sd,
    nrm, tok, info, sdb, gst, dst, dnb, rows, yst, est, hid, ret, cmb, farin, acc, shid,
    wbuf, dbuf, gcol,
    ld_sem, tk_ld, out_sem,
    tok_s, tok_r, info_s, info_r, sh_s, sh_r, shy_s, sd_s, sd_r, sdy_s,
    gu_s, gu_r, dn_s, dn_r, y_s, e_s, rows_r, x_s, part_s, part_r,
    hid_s, hid_r, shid_s, shid_r, edo_s, edo_r, sdo_s, sdo_r, ret_s, ret_r,
    cmb_r, far_s, far_r,
):
    E, Pn, C, Z, Y, half, per = S.E, S.P, S.C, S.Z, S.Y, S.half, S.per
    cap, Dc, Hc, Sc, nt = S.cap, S.Dc, S.Hc, S.Sc, S.nt
    f, t = lax.axis_index("fs"), lax.axis_index("tp")
    z, y = f // Y, f % Y
    x, c = t // cores, t % cores
    inner = (z > 0) & (z < Z - 1)
    to_low, to_high = z == 1, z == Z - 2

    def peer(k):
        span = Z // 2
        p = k // Y
        near = p // span
        plane = (z // span + 1 + near) % 2 * span + (z + p + near) % span
        return plane * Y + (y + 1 + k % Y) % Y

    def rcopy(src, dst, ssem, rsem, to):
        return pltpu.make_async_remote_copy(
            src_ref=src, dst_ref=dst, send_sem=ssem, recv_sem=rsem,
            device_id=to, device_id_type=MESH,
        )

    def arrived(ref, rsem):
        rcopy(ref, ref, out_sem.at[0], rsem, ((f + 1) % E, t)).wait_recv()

    def sent(ref, ssem):
        rcopy(ref, ref, ssem, out_sem.at[0], ((f + 1) % E, t)).wait_send()

    def loop(count, body, start=0):
        lax.fori_loop(start, count, lambda i, v: (body(i), v)[1], 0)

    def load_w(k, slot):
        e = peer(k)
        return [
            pltpu.make_async_copy(w.at[e], wbuf.at[slot, i], ld_sem.at[slot, i])
            for i, w in ((0, gate_t), (1, up_t))
        ]

    def load_d(k, slot):
        return pltpu.make_async_copy(down_t.at[peer(k)], dbuf.at[slot], ld_sem.at[slot, 2])

    tok_load = pltpu.make_async_copy(tokens, nrm, tk_ld.at[0])
    tok_load.start()
    sh_loads = [
        pltpu.make_async_copy(sgate_t, wbuf.at[1, 0], ld_sem.at[1, 0]),
        pltpu.make_async_copy(sup_t, wbuf.at[1, 1], ld_sem.at[1, 1]),
        pltpu.make_async_copy(sdown_t, dbuf.at[1], ld_sem.at[1, 2]),
    ]
    for copy in sh_loads + load_w(0, 0) + [load_d(0, 0)]:
        copy.start()
    greet = pltpu.get_barrier_semaphore()
    for i in range(1, E):
        pl.semaphore_signal(greet, inc=1, device_id=((f + i) % E, t), device_id_type=MESH)
    for i in range(1, Pn):
        pl.semaphore_signal(greet, inc=1, device_id=(f, (t + i) % Pn), device_id_type=MESH)

    T = S.T
    gcol[...] = jnp.broadcast_to(gain[...], (128, S.Dr)).T
    for copy in sh_loads:
        copy.wait()
    shb[f, :, 0:Sc] = (gcol[:, 0:1] * wbuf[1, 0]).astype(BF16)
    shb[f, :, Sc:] = (gcol[:, 0:1] * wbuf[1, 1]).astype(BF16)
    sdb[f] = dbuf[1].astype(BF16)

    by_z = lambda zs: zs
    by_f = lambda zs: zs * Y + y

    def lanes_of(slot_of, hop, within):
        low, high = (1, Z - 1) if within else (0, Z)
        for d in range(2):
            zs = z - hop if d == 0 else z + hop
            there = (zs >= 0) if d == 0 else (zs < Z)
            if within and hop:
                there &= inner
            onward = (z + 1 < high) if d == 0 else (z > low)
            yield d, there, onward, slot_of(jnp.clip(zs, 0, Z - 1)), f + Y if d == 0 else f - Y

    def line(buf, slot_of, ssem, rsem, hop, within=False):
        for d, there, onward, slot, nxt in lanes_of(slot_of, hop, within):

            @pl.when(there)
            def _():
                if hop:
                    arrived(buf.at[slot], rsem.at[slot])

                @pl.when(onward)
                def _():
                    rcopy(
                        buf.at[slot], buf.at[slot], ssem.at[d, hop], rsem.at[slot], (nxt, t)
                    ).start()

    def line_sent(buf, slot_of, ssem, hop, within=False):
        for d, there, onward, slot, nxt in lanes_of(slot_of, hop, within):

            @pl.when(there & onward)
            def _():
                sent(buf.at[slot], ssem.at[d, hop])


    def shared_y(zs):
        s = by_f(zs)
        for j in range(1, Y):
            to = (z * Y + (y + j) % Y, t)
            rcopy(shb.at[s], shb.at[s], shy_s.at[j - 1], sh_r.at[s], to).start()
            rcopy(sdb.at[s], sdb.at[s], sdy_s.at[j - 1], sd_r.at[s], to).start()

    def come(hop, act_on):
        for zs, there in ((z - hop, z - hop >= 0), (z + hop, z + hop < Z)):
            at = jnp.clip(zs, 0, Z - 1)

            @pl.when(there)
            def _():
                act_on(at)

    def shared_hop(hop):
        line(shb, by_f, sh_s, sh_r, hop)
        line(sdb, by_f, sd_s, sd_r, hop)
        if hop:
            come(hop, shared_y)
        else:
            shared_y(z)

    pl.semaphore_wait(greet, E + Pn - 2)
    shared_hop(0)
    wide = max(16, E)
    r0, r1 = route[0:1, :].astype(F32), route[1:2, :].astype(F32)
    names = lax.broadcasted_iota(jnp.int32, (wide, T), 0).astype(F32)
    hit0, hit1 = r0 == names, r1 == names
    chosen = (hit0 | hit1).astype(F32).astype(BF16)
    before = lax.broadcasted_iota(jnp.int32, (T, T), 0) < lax.broadcasted_iota(
        jnp.int32, (T, T), 1
    )
    count = jnp.dot(chosen, before.astype(F32).astype(BF16), preferred_element_type=F32)
    s0 = jnp.sum(jnp.where(hit0, count, 0.0), axis=0, keepdims=True)
    s1 = jnp.sum(jnp.where(hit1, count, 0.0), axis=0, keepdims=True)
    info[z, 0:1, :] = r0
    info[z, 1:2, :] = r1
    info[z, 2:3, :] = s0
    info[z, 3:4, :] = s1
    info[z, 4:6, :] = weight[...]

    tok_load.wait()
    tile = min(64, T)

    def normalise(i):
        at = pl.ds(pl.multiple_of(i * tile, tile), tile)
        v = nrm[at, :].astype(F32)
        v = v * lax.rsqrt(jnp.mean(v * v, axis=1, keepdims=True) + norm_eps)
        nrm[at, :] = v.astype(BF16)
        tok[z, at, :] = nrm[at, pl.ds(pl.multiple_of(t * Dc, Dc), Dc)]

    loop(T // tile, normalise)

    def tell(act_on):
        for i in range(1, Z):
            zo = (z + i) % Z

            @pl.when((zo > 0) & (zo < Z - 1))
            def _():
                act_on(i - 1, zo)

    tell(
        lambda i, zo: rcopy(
            info.at[z], info.at[z], info_s.at[i], info_r.at[z], (zo * Y + y, t)
        ).start()
    )
    line(tok, by_z, tok_s, tok_r, 0, True)

    def convert_gu(k):
        slot = k % 2
        for copy in load_w(k, slot):
            copy.wait()

        @pl.when(k + 1 < E)
        def _():
            for copy in load_w(k + 1, 1 - slot):
                copy.start()

        for i in range(2):
            gst[k, :, i * Hc : (i + 1) * Hc] = (gcol[:, 0:1] * wbuf[slot, i]).astype(BF16)

    def convert_dn(k):
        slot = k % 2
        load_d(k, slot).wait()

        @pl.when(k + 1 < E)
        def _():
            load_d(k + 1, 1 - slot).start()

        dst[k] = dbuf[slot].astype(BF16)

    def x_out(s):
        for i in range(1, C):
            to = (f, (x + i) % C * cores + c)
            rcopy(rows.at[t, s], rows.at[t, s], x_s.at[i - 1], rows_r.at[t, s], to).start()
        rcopy(rows.at[t, s], rows.at[t, s], part_s.at[0], part_r.at[0], (f, x * cores + 1 - c)).start()

    def picked(zs, e, put_block):
        e = e.astype(F32)
        slots = lax.broadcasted_iota(jnp.int32, (cap, T), 0).astype(F32)
        got = (info[zs, 0:1, :] == e) & (info[zs, 2:3, :] == slots)
        got |= (info[zs, 1:2, :] == e) & (info[zs, 3:4, :] == slots)
        got = got.astype(F32).astype(BF16)

        def part(n):
            at = pl.ds(pl.multiple_of(n * nt, nt), nt)
            put_block(at, jnp.dot(got, tok[zs, :, at], preferred_element_type=F32).astype(BF16))

        loop(Dc // nt, part)

    def pick(zs):
        s = by_f(zs)

        def for_end(zt):
            for j in range(Y):

                def put_block(at, block):
                    est[zs, j, :, at] = block

                picked(zs, zt * Y + (y + j) % Y, put_block)
            for j in range(Y):
                rcopy(
                    est.at[zs, j], rows.at[t, s], e_s.at[j], rows_r.at[t, s],
                    (zt * Y + (y + j) % Y, t),
                ).start()

        for zt, near in ((0, to_low), (Z - 1, to_high)):

            @pl.when(near & (zs != zt))
            def _():
                for_end(zt)

        for j in list(range(1, Y)) + [0]:

            def put_block(at, block):
                if j:
                    yst[zs, j - 1, :, at] = block
                else:
                    rows[t, s, :, at] = block

            picked(zs, z * Y + (y + j) % Y, put_block)
        for j in range(1, Y):
            to = (z * Y + (y + j) % Y, t)
            rcopy(
                yst.at[zs, j - 1], rows.at[t, s], y_s.at[j - 1], rows_r.at[t, s], to
            ).start()
        x_out(s)

    def send_gu(k):
        e = peer(k)
        rcopy(gst.at[k], gub.at[f], gu_s.at[k], gu_r.at[f], (e, t)).start()

    def send_dn(k):
        e = peer(k)
        rcopy(dst.at[k], dnb.at[f], dn_s.at[k], dn_r.at[f], (e, t)).start()

    def pick_come(at):
        arrived(info.at[at], info_r.at[at])
        pick(at)

    def tok_hop(hop):
        line(tok, by_z, tok_s, tok_r, hop, True)

        @pl.when(inner)
        def _():
            come(hop, pick_come)

    pick(z)
    loop(E, convert_gu)
    loop(E, convert_dn)
    gub[f] = gst[E - 1]
    dnb[f] = dst[E - 1]
    for hop in range(1, Z - 1):
        tok_hop(hop)
        shared_hop(hop)
        line_sent(tok, by_z, tok_s, hop - 1, True)
        line_sent(shb, by_f, sh_s, hop - 1)
        line_sent(sdb, by_f, sd_s, hop - 1)
    if Z == 2:
        line_sent(tok, by_z, tok_s, 0, True)
        line_sent(shb, by_f, sh_s, 0)
        line_sent(sdb, by_f, sd_s, 0)
    if Z > 2:
        line_sent(tok, by_z, tok_s, Z - 2, True)
    loop(half // 2, send_gu)
    loop(E - 1, send_gu, half)

    for i in range(Z):
        zs = jnp.where(z < Z // 2, z + i, z + Z - i) % Z
        for j in range(Y):
            s = zs * Y + (y + j) % Y
            if j:
                arrived(rows.at[t, s], rows_r.at[t, s])
                x_out(s)
            elif i:

                @pl.when(jnp.logical_not(inner))
                def _():
                    arrived(rows.at[t, s], rows_r.at[t, s])
                    x_out(s)

    loop(half // 2, lambda k: sent(gst.at[k], gu_s.at[k]))
    loop(half, send_gu, half // 2)
    loop(E - 1, send_dn, half)
    for i in range(1, C):
        to_t = (x + i) % C * cores + c

        def forward(s):
            arrived(rows.at[to_t, s], rows_r.at[to_t, s])
            rcopy(
                rows.at[to_t, s], rows.at[to_t, s], part_s.at[i], part_r.at[i],
                (f, x * cores + 1 - c),
            ).start()

        loop(E, forward)
    def put(src, dst_ref, i):
        copy = pltpu.make_async_copy(src, dst_ref, out_sem.at[i])
        copy.start()
        return copy

    puts = []
    own_cols = pl.ds(pl.multiple_of(t * Dc, Dc), Dc)

    def spread(buf, out, ssem, rsem, i):
        for k in range(1, Pn):
            tt = (t + k) % Pn
            rcopy(
                buf.at[pl.ds(tt * per, per)], out.at[:, :, own_cols], ssem.at[k - 1],
                rsem.at[t], (f, tt),
            ).start()
        return put(buf.at[pl.ds(t * per, per)], out.at[:, :, own_cols], i)

    def spread_wait(buf, out, ssem, rsem):
        for k in range(1, Pn):
            tt = (t + k) % Pn
            sent(buf.at[pl.ds(tt * per, per)], ssem.at[k - 1])
            at = pl.ds(pl.multiple_of(tt * Dc, Dc), Dc)
            arrived(out.at[:, :, at], rsem.at[tt])

    if Z > 2:
        shared_hop(Z - 1)
    loop(half, lambda k: sent(gst.at[k], gu_s.at[k]), half // 2)

    def act(v, width):
        gate, up = v[:, :width], v[:, width:]
        return (gate / (1.0 + jnp.exp(-gate)) * up).astype(BF16)

    mt = min(256, T)

    def shared_in(m):
        at = pl.ds(pl.multiple_of(m * mt, mt), mt)
        total = None
        for q in range(Pn):
            w = shb[q * per : (q + 1) * per].reshape(Dc, 2 * Sc)
            term = jnp.dot(nrm[at, q * Dc : (q + 1) * Dc], w, preferred_element_type=F32)
            total = term if total is None else total + term
        shid[t, at, :] = act(total, Sc)

    def inner_of(s):
        return (s // Y > 0) & (s // Y < Z - 1)

    def rows_waits():
        part = x * cores + 1 - c
        arrived(rows.at[part], part_r.at[0])
        for i in range(1, C):
            arrived(rows.at[(x + i) % C * cores + 1 - c], part_r.at[i])

    rows_waits()

    def wait_gu(k):
        s = peer(k)
        arrived(gub.at[s], gu_r.at[s])

    loop(E - 1, wait_gu)
    loop(half, send_dn)
    M, g, groups = S.M, S.g, S.groups
    own = f // g

    low = f < half
    side = groups // 2
    mid_z = jnp.where(low, Z // 2 - 1, Z // 2)
    over_z = jnp.where(low, Z // 2, Z // 2 - 1)

    def group_at(k):
        at = jnp.where(inner, k, side - 1 - k)
        far = jnp.where(low, groups - 1 - at, at)
        near = own // side * side + (own + 1 + k - side) % side
        return jnp.where(k < side, far, near)

    def hidden_in(k):
        q0 = group_at(k)
        span = pl.ds(q0 * g, g)
        total = None
        for q in range(Pn):
            w = gub[q * per : (q + 1) * per].reshape(Dc, 2 * Hc)
            term = jnp.dot(rows[q, span].reshape(M, Dc), w, preferred_element_type=F32)
            total = term if total is None else total + term
        hid[t, span] = act(total, Hc).reshape(g, cap, Hc)

    partner = x * cores + 1 - c

    def pass_hidden(i, tt, k, to):
        span = pl.ds(group_at(k) * g, g)
        rcopy(hid.at[tt, span], hid.at[tt, span], hid_s.at[i], hid_r.at[tt, k], (f, to)).start()

    def send_hidden(k):
        for i in range(1, C):
            pass_hidden(i, t, k, (x + i) % C * cores + c)
        pass_hidden(0, t, k, partner)

    def forward_hidden(k):
        span = pl.ds(group_at(k) * g, g)
        for i in range(1, C):
            tt = (x + i) % C * cores + c
            arrived(hid.at[tt, span], hid_r.at[tt, k])
            pass_hidden(C - 1 + i, tt, k, partner)

    def hidden_step(k):
        hidden_in(k)

        @pl.when(k > 0)
        def _():
            send_hidden(k - 1)

    loop(groups, hidden_step)

    def wait_dn(k):
        s = peer(k)
        arrived(dnb.at[s], dn_r.at[s])

    send_hidden(groups - 1)
    for j in range(1, Y):
        for zs in range(Z):
            s = zs * Y + (y + j) % Y
            arrived(shb.at[s], sh_r.at[s])
            arrived(sdb.at[s], sd_r.at[s])

    loop(T // mt, shared_in)

    for k in range(1, Pn):
        rcopy(shid.at[t], shid.at[t], shid_s.at[k - 1], shid_r.at[t], (f, (t + k) % Pn)).start()
    puts.append(spread(sdb, sd, sdo_s, sdo_r, 3))
    loop(groups, forward_hidden)
    loop(E - 1, wait_dn)

    def res_at(s):
        return tok.at[s // g, pl.ds(pl.multiple_of(s % g * cap, cap), cap)]

    def send_back(k):
        for i in range(g):
            s = group_at(k) * g + i
            over = (s // Y == over_z) & inner_of(s)
            to = mid_z * Y + s % Y

            @pl.when(over & (to != f))
            def _():
                rcopy(res_at(s), cmb.at[f % half], ret_s.at[s], cmb_r.at[f % half], (to, t)).start()

            @pl.when(jnp.logical_not(over) & (s != f))
            def _():
                rcopy(res_at(s), ret.at[f], ret_s.at[s], ret_r.at[f], (s, t)).start()

    def back_step(k):
        span = pl.ds(group_at(k) * g, g)

        for i in range(C):
            tt = (x + i) % C * cores + 1 - c
            arrived(hid.at[tt, span], hid_r.at[tt, k])

        def part(n):
            at = pl.ds(pl.multiple_of(n * nt, nt), nt)
            total = None
            for q in range(Pn):
                w = dnb[q * per : (q + 1) * per, :, at].reshape(Hc, nt)
                term = jnp.dot(hid[q, span].reshape(M, Hc), w, preferred_element_type=F32)
                total = term if total is None else total + term
            tok[group_at(k), 0:M, at] = total.astype(BF16)

        loop(Dc // nt, part)
        send_back(k)

    loop(groups, back_step)
    ret[f] = res_at(f)[...]

    def weigh(zs, base, many):
        spot = (lax.broadcasted_iota(jnp.int32, (many, T), 0) + base).astype(F32)
        at0 = info[zs, 0:1, :] * cap + info[zs, 2:3, :]
        at1 = info[zs, 1:2, :] * cap + info[zs, 3:4, :]
        share = jnp.where(at0 == spot, info[zs, 4:5, :], 0.0)
        share += jnp.where(at1 == spot, info[zs, 5:6, :], 0.0)
        return share.T.astype(BF16)

    puts.append(spread(dnb, ed, edo_s, edo_r, 6))
    @pl.when(inner)
    def _():
        to = over_z * Y + y
        cmb[f % half] = res_at(to)[...]
        for i in range(1, half):
            e = (f + i) % half
            arrived(cmb.at[e], cmb_r.at[e])
        many = half * cap
        shares = weigh(over_z, f // half * many, many)

        def part(n):
            at = pl.ds(pl.multiple_of(n * nt, nt), nt)
            block = cmb[:, :, at].reshape(many, nt)
            nrm[:, at] = jnp.dot(shares, block, preferred_element_type=F32).astype(BF16)

        loop(Dc // nt, part)
        rcopy(nrm.at[:, pl.ds(0, Dc)], farin, far_s.at[0], far_r.at[0], (to, t)).start()


    for k in range(1, Pn):
        arrived(shid.at[(t + k) % Pn], shid_r.at[(t + k) % Pn])

    def shared_out(n):
        at = pl.ds(pl.multiple_of(n * nt, nt), nt)
        total = None
        for q in range(Pn):
            w = sdb[q * per : (q + 1) * per, :, at].reshape(Sc, nt)
            term = jnp.dot(shid[q], w, preferred_element_type=F32)
            total = term if total is None else total + term
        acc[:, at] = total

    loop(Dc // nt, shared_out)


    def combine(k):
        q0 = group_at(groups - 1 - k)
        for j in range(g):
            s = q0 * g + j

            @pl.when(s != f)
            def _():
                arrived(ret.at[s], ret_r.at[s])

        shares = weigh(z, q0 * M, M)

        def part(n):
            at = pl.ds(pl.multiple_of(n * nt, nt), nt)
            block = ret[pl.ds(q0 * g, g), :, at].reshape(M, nt)
            acc[:, at] += jnp.dot(shares, block, preferred_element_type=F32)

        loop(Dc // nt, part)

    loop(side, combine)

    @pl.when(jnp.logical_not(inner))
    def _():
        loop(groups, combine, side)

    @pl.when(inner)
    def _():
        arrived(farin, far_r.at[0])
        acc[...] += farin[...].astype(F32)

    outb[...] = acc[...].astype(BF16)

    if Z > 2:
        line_sent(shb, by_f, sh_s, Z - 2)
        line_sent(sdb, by_f, sd_s, Z - 2)
    tell(lambda i, zo: sent(info.at[z], info_s.at[i]))
    for j in range(1, Y):
        sent(shb.at[pl.ds(0, Z)], shy_s.at[j - 1])
        sent(sdb.at[pl.ds(0, Z)], sdy_s.at[j - 1])

        @pl.when(inner)
        def _():
            sent(yst.at[:, j - 1], y_s.at[j - 1])

        @pl.when(jnp.logical_not(inner))
        def _():
            sent(yst.at[0, j - 1], y_s.at[j - 1])

    @pl.when(to_low | to_high)
    def _():
        for j in range(Y):
            sent(est.at[pl.ds(0, Z - 1), j], e_s.at[j])

    for i in range(1, C):
        sent(rows.at[t], x_s.at[i - 1])
    for i in range(C):
        sent(rows.at[t], part_s.at[i])
    loop(E - 1, lambda k: sent(gst.at[k], gu_s.at[k]), half)
    loop(E - 1, lambda k: sent(dst.at[k], dn_s.at[k]))
    for k in range(1, Pn):
        sent(shid.at[t], shid_s.at[k - 1])
        sent(hid.at[t], hid_s.at[k - 1])

    def drain_ret(k):
        s = peer(k)

        @pl.when(jnp.logical_not(inner & (s == over_z * Y + y)))
        def _():
            sent(res_at(s), ret_s.at[s])

    @pl.when(inner)
    def _():
        sent(nrm.at[:, pl.ds(0, Dc)], far_s.at[0])

    loop(E - 1, drain_ret)
    spread_wait(sdb, sd, sdo_s, sdo_r)
    spread_wait(dnb, ed, edo_s, edo_r)
    for copy in puts:
        copy.wait()


def handed(S, gub, shb, outb, ed, sd, eg, eu, sg, su, mixed, ed_out, sd_out, held, kept, sem):
    Hc, Sc = S.Hc, S.Sc
    loads = [
        pltpu.make_async_copy(ed, held, sem.at[0]),
        pltpu.make_async_copy(sd, kept, sem.at[1]),
    ]
    stores = [
        pltpu.make_async_copy(gub.at[:, :, pl.ds(0, Hc)], eg, sem.at[2]),
        pltpu.make_async_copy(gub.at[:, :, pl.ds(Hc, Hc)], eu, sem.at[3]),
        pltpu.make_async_copy(shb.at[:, :, pl.ds(0, Sc)], sg, sem.at[4]),
        pltpu.make_async_copy(shb.at[:, :, pl.ds(Sc, Sc)], su, sem.at[5]),
        pltpu.make_async_copy(outb, mixed, sem.at[6]),
    ]
    for copy in loads + stores:
        copy.start()
    for i, (load, buf, out) in enumerate(zip(loads, (held, kept), (ed_out, sd_out))):
        load.wait()
        store = pltpu.make_async_copy(buf, out, sem.at[7 + i])
        store.start()
        stores.append(store)
    for copy in stores:
        copy.wait()


def on_device(
    tokens, norm_gain, gate_train, up_train, down_train,
    shared_gate_train, shared_up_train, shared_down_train, route_expert, route_weight,
):
    S = Sizes(
        lax.axis_size("fs"), lax.axis_size("tp"), tokens.shape, gate_train.shape,
        down_train.shape, shared_gate_train.shape, shared_down_train.shape,
        route_expert.shape[1],
    )
    E, Pn, C, Z, Y = S.E, S.P, S.C, S.Z, S.Y
    T, D, cap, Dr, Hc, Hr, Dc, Sc, Sr, per = (
        S.T, S.D, S.cap, S.Dr, S.Hc, S.Hr, S.Dc, S.Sc, S.Sr, S.per
    )
    dma = pltpu.SemaphoreType.DMA
    anywhere = pl.BlockSpec(memory_space=pl.ANY)
    inside = pl.BlockSpec(memory_space=pltpu.VMEM)
    far = max(1, Y - 1)
    scratch = [
        pltpu.VMEM((T, D), BF16),
        pltpu.VMEM((Z, T, Dc), BF16),
        pltpu.VMEM((Z, 8, T), F32),
        pltpu.VMEM((E, Sr, Dc), BF16),
        pltpu.VMEM((E, Dr, 2 * Hc), BF16),
        pltpu.VMEM((E, Hr, Dc), BF16),
        pltpu.VMEM((E, Hr, Dc), BF16),
        pltpu.VMEM((Pn, E, cap, Dc), BF16),
        pltpu.VMEM((Z, far, cap, Dc), BF16),
        pltpu.VMEM((Z, Y, cap, Dc), BF16),
        pltpu.VMEM((Pn, E, cap, Hc), BF16),
        pltpu.VMEM((E, cap, Dc), BF16),
        pltpu.VMEM((E // 2, cap, Dc), BF16),
        pltpu.VMEM((T, Dc), BF16),
        pltpu.VMEM((T, Dc), F32),
        pltpu.VMEM((Pn, T, Sc), BF16),
        pltpu.VMEM((2, 2, Dr, Hc), F32),
        pltpu.VMEM((2, Hr, Dc), F32),
        pltpu.VMEM((Dr, 128), F32),
        dma((2, 3)), dma((1,)), dma((8,)),
        dma((2, Z)), dma((Z,)), dma((Z,)), dma((Z,)),
        dma((2, Z)), dma((E,)), dma((far,)),
        dma((2, Z)), dma((E,)), dma((far,)),
        dma((E,)), dma((E,)), dma((E,)), dma((E,)),
        dma((far,)), dma((Y,)), dma((Pn, E)), dma((C,)), dma((C,)), dma((C,)),
        dma((Pn,)), dma((Pn, S.groups)), dma((Pn,)), dma((Pn,)),
        dma((Pn,)), dma((Pn,)), dma((Pn,)), dma((Pn,)),
        dma((E,)), dma((E,)),
        dma((E // 2,)), dma((1,)), dma((1,)),
    ]
    shape = lambda *dims: jax.ShapeDtypeStruct(dims, BF16)
    flops = 2 * T * D * 2 * Sc + 2 * E * cap * D * 2 * Hc + 4 * E * cap * D * Hc
    vmem = pltpu.MemorySpace.VMEM
    handed_on = [(E, Dr, 2 * Hc), (E, Dr, 2 * Sc), (T, Dc)]
    limit = 66781184 - 2 * sum(math.prod(dims) for dims in handed_on)
    outs = pl.pallas_call(
        functools.partial(kernel, S),
        out_shape=[vmem(dims, BF16) for dims in handed_on]
        + [shape(per, Hr, D), shape(per, Sr, D)],
        in_specs=[anywhere] * 7 + [inside] * 3,
        out_specs=[inside] * 3 + [anywhere] * 2,
        scratch_shapes=scratch,
        compiler_params=pltpu.CompilerParams(
            collective_id=0, has_side_effects=True, vmem_limit_bytes=limit
        ),
        cost_estimate=pl.CostEstimate(flops=flops, bytes_accessed=1 << 26, transcendentals=0),
    )(
        tokens, gate_train, up_train, down_train, shared_gate_train, shared_up_train,
        shared_down_train, norm_gain[None, :], route_expert.T, route_weight.T,
    )
    eg, eu, sg, su, mixed, ed, sd = pl.pallas_call(
        functools.partial(handed, S),
        out_shape=[
            shape(E, Dr, Hc), shape(E, Dr, Hc), shape(E, Dr, Sc), shape(E, Dr, Sc),
            shape(T, Dc), shape(per, Hr, D), shape(per, Sr, D),
        ],
        in_specs=[inside] * 3 + [anywhere] * 2,
        out_specs=[anywhere] * 7,
        scratch_shapes=[
            pltpu.VMEM((per, Hr, D), BF16), pltpu.VMEM((per, Sr, D), BF16), dma((9,))
        ],
        compiler_params=pltpu.CompilerParams(vmem_limit_bytes=1 << 25),
    )(
        *[pltpu.with_memory_space_constraint(o, vmem) for o in outs[:3]],
        *[pltpu.with_memory_space_constraint(o, pltpu.MemorySpace.HBM) for o in outs[3:]],
    )
    return (
        eg.reshape(1, D, Hc), eu.reshape(1, D, Hc), ed.reshape(1, per * Hr, D),
        sg.reshape(D, Sc), su.reshape(D, Sc), sd.reshape(per * Sr, D), mixed,
    )


def solution(mesh):
    placed = (
        P("fs", None),
        P("fs"),
        P(None, "fs", "tp"),
        P(None, "fs", "tp"),
        P(None, "fs", "tp"),
        P("fs", "tp"),
        P("fs", "tp"),
        P("fs", "tp"),
        P("fs", None),
        P("fs", None),
    )
    return jax.shard_map(
        on_device,
        mesh=mesh,
        in_specs=placed,
        out_specs=(
            P("fs", None, "tp"),
            P("fs", None, "tp"),
            P("fs", "tp", None),
            P(None, "tp"),
            P(None, "tp"),
            P("tp", None),
            P("fs", "tp"),
        ),
        check_vma=False,
    )
```

```python
import functools
import math

import jax
import jax.numpy as jnp
from jax import lax
from jax.experimental import pallas as pl
from jax.experimental.pallas import tpu as pltpu
from jax.sharding import PartitionSpec as P

norm_eps = 1e-06
cores = 2
MESH = pl.DeviceIdType.MESH
F32, BF16 = jnp.float32, jnp.bfloat16


class Sizes:
    def __init__(self, experts, pieces, tokens, gate, down, sgate, sdown, top):
        self.E, self.P = experts, pieces
        self.C = pieces // cores
        long = 1
        while long * long < experts:
            long *= 2
        self.Z, self.Y = long, experts // long
        self.half = experts // 2
        self.T, self.D = tokens
        self.cap = 3 * self.T * top // (2 * experts)
        self.Dr, self.Hc = gate[1:]
        self.Hr, self.Dc = down[1:]
        self.Dr2, self.Sc = sgate
        self.Sr = sdown[0]
        self.per = experts // pieces
        self.g = 1
        while self.g * self.cap % 128:
            self.g *= 2
        self.groups = experts // self.g
        self.M = self.g * self.cap
        self.nt = min(256, self.Dc)
        assert self.groups <= self.Z and self.M <= self.T


def kernel(
    S,
    tokens, gate_t, up_t, down_t, sgate_t, sup_t, sdown_t, gain, route, weight,
    gub, shb, outb, ed, sd,
    nrm, tok, info, sdb, gst, dst, dnb, rows, yst, est, hid, ret, cmb, farin, acc, shid,
    dbuf, gcol,
    ld_sem, tk_ld, out_sem,
    tok_s, tok_r, info_s, info_r, sh_s, sh_r, shy_s, sd_s, sd_r, sdy_s,
    gu_s, gu_r, dn_s, dn_r, y_s, e_s, rows_r, x_s, part_s, part_r,
    hid_s, hid_r, shid_s, shid_r, edo_s, edo_r, sdo_s, sdo_r, ret_s, ret_r,
    cmb_r, far_s, far_r,
):
    E, Pn, C, Z, Y, half, per = S.E, S.P, S.C, S.Z, S.Y, S.half, S.per
    cap, Dc, Hc, Sc, nt = S.cap, S.Dc, S.Hc, S.Sc, S.nt
    f, t = lax.axis_index("fs"), lax.axis_index("tp")
    z, y = f // Y, f % Y
    x, c = t // cores, t % cores
    inner = (z > 0) & (z < Z - 1)
    to_low, to_high = z == 1, z == Z - 2

    def peer(k):
        span = Z // 2
        p = k // Y
        near = p // span
        plane = (z // span + 1 + near) % 2 * span + (z + p + near) % span
        return plane * Y + (y + 1 + k % Y) % Y

    def rcopy(src, dst, ssem, rsem, to):
        return pltpu.make_async_remote_copy(
            src_ref=src, dst_ref=dst, send_sem=ssem, recv_sem=rsem,
            device_id=to, device_id_type=MESH,
        )

    def arrived(ref, rsem):
        rcopy(ref, ref, out_sem.at[0], rsem, ((f + 1) % E, t)).wait_recv()

    def sent(ref, ssem):
        rcopy(ref, ref, ssem, out_sem.at[0], ((f + 1) % E, t)).wait_send()

    def loop(count, body, start=0):
        lax.fori_loop(start, count, lambda i, v: (body(i), v)[1], 0)

    def passing(slot, i):
        at = pl.multiple_of((slot * 2 + i) * Hc, Hc)
        return acc.at[pl.ds(0, S.Dr), pl.ds(at, Hc)]

    def load_w(k, slot):
        e = peer(k)
        return [
            pltpu.make_async_copy(w.at[e], passing(slot, i), ld_sem.at[slot, i])
            for i, w in ((0, gate_t), (1, up_t))
        ]

    def load_d(k, slot):
        return pltpu.make_async_copy(down_t.at[peer(k)], dbuf.at[slot], ld_sem.at[slot, 2])

    tok_load = pltpu.make_async_copy(tokens, nrm, tk_ld.at[0])
    tok_load.start()
    sh_loads = [
        pltpu.make_async_copy(sgate_t, passing(1, 0), ld_sem.at[1, 0]),
        pltpu.make_async_copy(sup_t, passing(1, 1), ld_sem.at[1, 1]),
        pltpu.make_async_copy(sdown_t, dbuf.at[1], ld_sem.at[1, 2]),
    ]
    for copy in sh_loads + load_w(0, 0) + [load_d(0, 0)]:
        copy.start()
    greet = pltpu.get_barrier_semaphore()
    for i in range(1, E):
        pl.semaphore_signal(greet, inc=1, device_id=((f + i) % E, t), device_id_type=MESH)
    for i in range(1, Pn):
        pl.semaphore_signal(greet, inc=1, device_id=(f, (t + i) % Pn), device_id_type=MESH)

    T = S.T
    gcol[...] = jnp.broadcast_to(gain[...], (128, S.Dr)).T
    for copy in sh_loads:
        copy.wait()
    shb[f, :, 0:Sc] = (gcol[:, 0:1] * passing(1, 0)[...]).astype(BF16)
    shb[f, :, Sc:] = (gcol[:, 0:1] * passing(1, 1)[...]).astype(BF16)
    sdb[f] = dbuf[1].astype(BF16)

    by_z = lambda zs: zs
    by_f = lambda zs: zs * Y + y

    def lanes_of(slot_of, hop, within):
        low, high = (1, Z - 1) if within else (0, Z)
        for d in range(2):
            zs = z - hop if d == 0 else z + hop
            there = (zs >= 0) if d == 0 else (zs < Z)
            if within and hop:
                there &= inner
            onward = (z + 1 < high) if d == 0 else (z > low)
            yield d, there, onward, slot_of(jnp.clip(zs, 0, Z - 1)), f + Y if d == 0 else f - Y

    def line(buf, slot_of, ssem, rsem, hop, within=False):
        for d, there, onward, slot, nxt in lanes_of(slot_of, hop, within):

            @pl.when(there)
            def _():
                if hop:
                    arrived(buf.at[slot], rsem.at[slot])

                @pl.when(onward)
                def _():
                    rcopy(
                        buf.at[slot], buf.at[slot], ssem.at[d, hop], rsem.at[slot], (nxt, t)
                    ).start()

    def line_sent(buf, slot_of, ssem, hop, within=False):
        for d, there, onward, slot, nxt in lanes_of(slot_of, hop, within):

            @pl.when(there & onward)
            def _():
                sent(buf.at[slot], ssem.at[d, hop])


    def shared_y(zs):
        s = by_f(zs)
        for j in range(1, Y):
            to = (z * Y + (y + j) % Y, t)
            rcopy(shb.at[s], shb.at[s], shy_s.at[j - 1], sh_r.at[s], to).start()
            rcopy(sdb.at[s], sdb.at[s], sdy_s.at[j - 1], sd_r.at[s], to).start()

    def come(hop, act_on):
        for zs, there in ((z - hop, z - hop >= 0), (z + hop, z + hop < Z)):
            at = jnp.clip(zs, 0, Z - 1)

            @pl.when(there)
            def _():
                act_on(at)

    def shared_hop(hop):
        line(shb, by_f, sh_s, sh_r, hop)
        line(sdb, by_f, sd_s, sd_r, hop)
        if hop:
            come(hop, shared_y)
        else:
            shared_y(z)

    pl.semaphore_wait(greet, E + Pn - 2)
    shared_hop(0)
    wide = max(16, E)
    r0, r1 = route[0:1, :].astype(F32), route[1:2, :].astype(F32)
    names = lax.broadcasted_iota(jnp.int32, (wide, T), 0).astype(F32)
    hit0, hit1 = r0 == names, r1 == names
    chosen = (hit0 | hit1).astype(F32).astype(BF16)
    before = lax.broadcasted_iota(jnp.int32, (T, T), 0) < lax.broadcasted_iota(
        jnp.int32, (T, T), 1
    )
    count = jnp.dot(chosen, before.astype(F32).astype(BF16), preferred_element_type=F32)
    s0 = jnp.sum(jnp.where(hit0, count, 0.0), axis=0, keepdims=True)
    s1 = jnp.sum(jnp.where(hit1, count, 0.0), axis=0, keepdims=True)
    info[z, 0:1, :] = r0
    info[z, 1:2, :] = r1
    info[z, 2:3, :] = s0
    info[z, 3:4, :] = s1
    info[z, 4:6, :] = weight[...]

    tok_load.wait()
    tile = min(64, T)

    def normalise(i):
        at = pl.ds(pl.multiple_of(i * tile, tile), tile)
        v = nrm[at, :].astype(F32)
        v = v * lax.rsqrt(jnp.mean(v * v, axis=1, keepdims=True) + norm_eps)
        nrm[at, :] = v.astype(BF16)
        tok[z, at, :] = nrm[at, pl.ds(pl.multiple_of(t * Dc, Dc), Dc)]

    loop(T // tile, normalise)

    def tell(act_on):
        for i in range(1, Z):
            zo = (z + i) % Z

            @pl.when((zo > 0) & (zo < Z - 1))
            def _():
                act_on(i - 1, zo)

    tell(
        lambda i, zo: rcopy(
            info.at[z], info.at[z], info_s.at[i], info_r.at[z], (zo * Y + y, t)
        ).start()
    )
    line(tok, by_z, tok_s, tok_r, 0, True)

    def convert_gu(k):
        slot = k % 2
        for copy in load_w(k, slot):
            copy.wait()

        @pl.when(k + 1 < E)
        def _():
            for copy in load_w(k + 1, 1 - slot):
                copy.start()

        for i in range(2):
            gst[k, :, i * Hc : (i + 1) * Hc] = (gcol[:, 0:1] * passing(slot, i)[...]).astype(BF16)

    def convert_dn(k):
        slot = k % 2
        load_d(k, slot).wait()

        @pl.when(k + 1 < E)
        def _():
            load_d(k + 1, 1 - slot).start()

        dst[k] = dbuf[slot].astype(BF16)

    def x_out(s):
        for i in range(1, C):
            to = (f, (x + i) % C * cores + c)
            rcopy(rows.at[t, s], rows.at[t, s], x_s.at[i - 1], rows_r.at[t, s], to).start()
        rcopy(rows.at[t, s], rows.at[t, s], part_s.at[0], part_r.at[0], (f, x * cores + 1 - c)).start()

    def picked(zs, e, put_block):
        e = e.astype(F32)
        slots = lax.broadcasted_iota(jnp.int32, (cap, T), 0).astype(F32)
        got = (info[zs, 0:1, :] == e) & (info[zs, 2:3, :] == slots)
        got |= (info[zs, 1:2, :] == e) & (info[zs, 3:4, :] == slots)
        got = got.astype(F32).astype(BF16)

        def part(n):
            at = pl.ds(pl.multiple_of(n * nt, nt), nt)
            put_block(at, jnp.dot(got, tok[zs, :, at], preferred_element_type=F32).astype(BF16))

        loop(Dc // nt, part)

    def pick(zs):
        s = by_f(zs)

        def for_end(zt):
            for j in range(Y):

                def put_block(at, block):
                    est[zs, j, :, at] = block

                picked(zs, zt * Y + (y + j) % Y, put_block)
            for j in range(Y):
                rcopy(
                    est.at[zs, j], rows.at[t, s], e_s.at[j], rows_r.at[t, s],
                    (zt * Y + (y + j) % Y, t),
                ).start()

        for zt, near in ((0, to_low), (Z - 1, to_high)):

            @pl.when(near & (zs != zt))
            def _():
                for_end(zt)

        for j in list(range(1, Y)) + [0]:

            def put_block(at, block):
                if j:
                    yst[zs, j - 1, :, at] = block
                else:
                    rows[t, s, :, at] = block

            picked(zs, z * Y + (y + j) % Y, put_block)
        for j in range(1, Y):
            to = (z * Y + (y + j) % Y, t)
            rcopy(
                yst.at[zs, j - 1], rows.at[t, s], y_s.at[j - 1], rows_r.at[t, s], to
            ).start()
        x_out(s)

    def send_gu(k):
        e = peer(k)
        rcopy(gst.at[k], gub.at[f], gu_s.at[k], gu_r.at[f], (e, t)).start()

    def send_dn(k):
        e = peer(k)
        rcopy(dst.at[k], dnb.at[f], dn_s.at[k], dn_r.at[f], (e, t)).start()

    def pick_come(at):
        arrived(info.at[at], info_r.at[at])
        pick(at)

    def tok_hop(hop):
        line(tok, by_z, tok_s, tok_r, hop, True)

        @pl.when(inner)
        def _():
            come(hop, pick_come)

    pick(z)
    loop(E, convert_gu)
    loop(E, convert_dn)
    gub[f] = gst[E - 1]
    dnb[f] = dst[E - 1]
    for hop in range(1, Z - 1):
        tok_hop(hop)
        shared_hop(hop)
        line_sent(tok, by_z, tok_s, hop - 1, True)
        line_sent(shb, by_f, sh_s, hop - 1)
        line_sent(sdb, by_f, sd_s, hop - 1)
    if Z == 2:
        line_sent(tok, by_z, tok_s, 0, True)
        line_sent(shb, by_f, sh_s, 0)
        line_sent(sdb, by_f, sd_s, 0)
    if Z > 2:
        line_sent(tok, by_z, tok_s, Z - 2, True)
    loop(half // 2, send_gu)
    loop(E - 1, send_gu, half)

    for i in range(Z):
        zs = jnp.where(z < Z // 2, z + i, z + Z - i) % Z
        for j in range(Y):
            s = zs * Y + (y + j) % Y
            if j:
                arrived(rows.at[t, s], rows_r.at[t, s])
                x_out(s)
            elif i:

                @pl.when(jnp.logical_not(inner))
                def _():
                    arrived(rows.at[t, s], rows_r.at[t, s])
                    x_out(s)

    loop(half // 2, lambda k: sent(gst.at[k], gu_s.at[k]))
    loop(half, send_gu, half // 2)
    loop(E - 1, send_dn, half)
    for i in range(1, C):
        to_t = (x + i) % C * cores + c

        def forward(s):
            arrived(rows.at[to_t, s], rows_r.at[to_t, s])
            rcopy(
                rows.at[to_t, s], rows.at[to_t, s], part_s.at[i], part_r.at[i],
                (f, x * cores + 1 - c),
            ).start()

        loop(E, forward)
    own_cols = pl.ds(pl.multiple_of(t * Dc, Dc), Dc)

    def spread(buf, out, ssem, rsem):
        for k in range(1, Pn):
            tt = (t + k) % Pn
            rcopy(
                buf.at[pl.ds(tt * per, per)], out.at[:, :, own_cols], ssem.at[k - 1],
                rsem.at[t], (f, tt),
            ).start()
        out[:, :, own_cols] = buf[pl.ds(t * per, per)]

    def spread_wait(buf, out, ssem, rsem):
        for k in range(1, Pn):
            tt = (t + k) % Pn
            sent(buf.at[pl.ds(tt * per, per)], ssem.at[k - 1])
            at = pl.ds(pl.multiple_of(tt * Dc, Dc), Dc)
            arrived(out.at[:, :, at], rsem.at[tt])

    if Z > 2:
        shared_hop(Z - 1)
    loop(half, lambda k: sent(gst.at[k], gu_s.at[k]), half // 2)

    def act(v, width):
        gate, up = v[:, :width], v[:, width:]
        return (gate / (1.0 + jnp.exp(-gate)) * up).astype(BF16)

    mt = min(256, T)

    def shared_in(m):
        at = pl.ds(pl.multiple_of(m * mt, mt), mt)
        total = None
        for q in range(Pn):
            w = shb[q * per : (q + 1) * per].reshape(Dc, 2 * Sc)
            term = jnp.dot(nrm[at, q * Dc : (q + 1) * Dc], w, preferred_element_type=F32)
            total = term if total is None else total + term
        shid[t, at, :] = act(total, Sc)

    def inner_of(s):
        return (s // Y > 0) & (s // Y < Z - 1)

    def rows_waits():
        part = x * cores + 1 - c
        arrived(rows.at[part], part_r.at[0])
        for i in range(1, C):
            arrived(rows.at[(x + i) % C * cores + 1 - c], part_r.at[i])

    rows_waits()

    def wait_gu(k):
        s = peer(k)
        arrived(gub.at[s], gu_r.at[s])

    loop(E - 1, wait_gu)
    loop(half, send_dn)
    M, g, groups = S.M, S.g, S.groups
    own = f // g

    low = f < half
    side = groups // 2
    mid_z = jnp.where(low, Z // 2 - 1, Z // 2)
    over_z = jnp.where(low, Z // 2, Z // 2 - 1)

    def group_at(k):
        at = jnp.where(inner, k, side - 1 - k)
        far = jnp.where(low, groups - 1 - at, at)
        near = own // side * side + (own + 1 + k - side) % side
        return jnp.where(k < side, far, near)

    def hidden_in(k):
        q0 = group_at(k)
        span = pl.ds(q0 * g, g)
        total = None
        for q in range(Pn):
            w = gub[q * per : (q + 1) * per].reshape(Dc, 2 * Hc)
            term = jnp.dot(rows[q, span].reshape(M, Dc), w, preferred_element_type=F32)
            total = term if total is None else total + term
        hid[t, span] = act(total, Hc).reshape(g, cap, Hc)

    partner = x * cores + 1 - c

    def pass_hidden(i, tt, k, to):
        span = pl.ds(group_at(k) * g, g)
        rcopy(hid.at[tt, span], hid.at[tt, span], hid_s.at[i], hid_r.at[tt, k], (f, to)).start()

    def send_hidden(k):
        for i in range(1, C):
            pass_hidden(i, t, k, (x + i) % C * cores + c)
        pass_hidden(0, t, k, partner)

    def forward_hidden(k):
        span = pl.ds(group_at(k) * g, g)
        for i in range(1, C):
            tt = (x + i) % C * cores + c
            arrived(hid.at[tt, span], hid_r.at[tt, k])
            pass_hidden(C - 1 + i, tt, k, partner)

    def hidden_step(k):
        hidden_in(k)

        @pl.when(k > 0)
        def _():
            send_hidden(k - 1)

    loop(groups, hidden_step)

    def wait_dn(k):
        s = peer(k)
        arrived(dnb.at[s], dn_r.at[s])

    send_hidden(groups - 1)
    for j in range(1, Y):
        for zs in range(Z):
            s = zs * Y + (y + j) % Y
            arrived(shb.at[s], sh_r.at[s])
            arrived(sdb.at[s], sd_r.at[s])

    loop(T // mt, shared_in)

    for k in range(1, Pn):
        rcopy(shid.at[t], shid.at[t], shid_s.at[k - 1], shid_r.at[t], (f, (t + k) % Pn)).start()
    spread(sdb, sd, sdo_s, sdo_r)
    loop(groups, forward_hidden)
    loop(E - 1, wait_dn)

    def res_at(s):
        return tok.at[s // g, pl.ds(pl.multiple_of(s % g * cap, cap), cap)]

    def send_back(k):
        for i in range(g):
            s = group_at(k) * g + i
            over = (s // Y == over_z) & inner_of(s)
            to = mid_z * Y + s % Y

            @pl.when(over & (to != f))
            def _():
                rcopy(res_at(s), cmb.at[f % half], ret_s.at[s], cmb_r.at[f % half], (to, t)).start()

            @pl.when(jnp.logical_not(over) & (s != f))
            def _():
                rcopy(res_at(s), ret.at[f], ret_s.at[s], ret_r.at[f], (s, t)).start()

    def back_step(k):
        span = pl.ds(group_at(k) * g, g)

        for i in range(C):
            tt = (x + i) % C * cores + 1 - c
            arrived(hid.at[tt, span], hid_r.at[tt, k])

        def part(n):
            at = pl.ds(pl.multiple_of(n * nt, nt), nt)
            total = None
            for q in range(Pn):
                w = dnb[q * per : (q + 1) * per, :, at].reshape(Hc, nt)
                term = jnp.dot(hid[q, span].reshape(M, Hc), w, preferred_element_type=F32)
                total = term if total is None else total + term
            tok[group_at(k), 0:M, at] = total.astype(BF16)

        loop(Dc // nt, part)
        send_back(k)

    loop(groups, back_step)
    ret[f] = res_at(f)[...]

    def weigh(zs, base, many):
        spot = (lax.broadcasted_iota(jnp.int32, (many, T), 0) + base).astype(F32)
        at0 = info[zs, 0:1, :] * cap + info[zs, 2:3, :]
        at1 = info[zs, 1:2, :] * cap + info[zs, 3:4, :]
        share = jnp.where(at0 == spot, info[zs, 4:5, :], 0.0)
        share += jnp.where(at1 == spot, info[zs, 5:6, :], 0.0)
        return share.T.astype(BF16)

    spread(dnb, ed, edo_s, edo_r)
    @pl.when(inner)
    def _():
        to = over_z * Y + y
        cmb[f % half] = res_at(to)[...]
        for i in range(1, half):
            e = (f + i) % half
            arrived(cmb.at[e], cmb_r.at[e])
        many = half * cap
        shares = weigh(over_z, f // half * many, many)

        def part(n):
            at = pl.ds(pl.multiple_of(n * nt, nt), nt)
            block = cmb[:, :, at].reshape(many, nt)
            nrm[:, at] = jnp.dot(shares, block, preferred_element_type=F32).astype(BF16)

        loop(Dc // nt, part)
        rcopy(nrm.at[:, pl.ds(0, Dc)], farin, far_s.at[0], far_r.at[0], (to, t)).start()


    for k in range(1, Pn):
        arrived(shid.at[(t + k) % Pn], shid_r.at[(t + k) % Pn])

    def shared_out(n):
        at = pl.ds(pl.multiple_of(n * nt, nt), nt)
        total = None
        for q in range(Pn):
            w = sdb[q * per : (q + 1) * per, :, at].reshape(Sc, nt)
            term = jnp.dot(shid[q], w, preferred_element_type=F32)
            total = term if total is None else total + term
        acc[:, at] = total

    loop(Dc // nt, shared_out)


    def combine(k):
        q0 = group_at(groups - 1 - k)
        shares = weigh(z, q0 * M, M)
        for j in range(g):
            s = q0 * g + j

            @pl.when(s != f)
            def _():
                arrived(ret.at[s], ret_r.at[s])


        def part(n):
            at = pl.ds(pl.multiple_of(n * nt, nt), nt)
            block = ret[pl.ds(q0 * g, g), :, at].reshape(M, nt)
            acc[:, at] += jnp.dot(shares, block, preferred_element_type=F32)

        loop(Dc // nt, part)

    if Z > 2:
        line_sent(shb, by_f, sh_s, Z - 2)
        line_sent(sdb, by_f, sd_s, Z - 2)
    tell(lambda i, zo: sent(info.at[z], info_s.at[i]))
    for j in range(1, Y):
        sent(shb.at[pl.ds(0, Z)], shy_s.at[j - 1])
        sent(sdb.at[pl.ds(0, Z)], sdy_s.at[j - 1])

        @pl.when(inner)
        def _():
            sent(yst.at[:, j - 1], y_s.at[j - 1])

        @pl.when(jnp.logical_not(inner))
        def _():
            sent(yst.at[0, j - 1], y_s.at[j - 1])

    @pl.when(to_low | to_high)
    def _():
        for j in range(Y):
            sent(est.at[pl.ds(0, Z - 1), j], e_s.at[j])

    for i in range(1, C):
        sent(rows.at[t], x_s.at[i - 1])
    for i in range(C):
        sent(rows.at[t], part_s.at[i])
    loop(E - 1, lambda k: sent(gst.at[k], gu_s.at[k]), half)
    loop(E - 1, lambda k: sent(dst.at[k], dn_s.at[k]))
    loop(side, combine)

    @pl.when(jnp.logical_not(inner))
    def _():
        loop(groups, combine, side)
        outb[...] = acc[...].astype(BF16)

    @pl.when(inner)
    def _():
        arrived(farin, far_r.at[0])
        outb[...] = (acc[...] + farin[...].astype(F32)).astype(BF16)


    for k in range(1, Pn):
        sent(shid.at[t], shid_s.at[k - 1])
        sent(hid.at[t], hid_s.at[k - 1])

    def drain_ret(k):
        s = peer(k)

        @pl.when(jnp.logical_not(inner & (s == over_z * Y + y)))
        def _():
            sent(res_at(s), ret_s.at[s])

    @pl.when(inner)
    def _():
        sent(nrm.at[:, pl.ds(0, Dc)], far_s.at[0])

    loop(E - 1, drain_ret)
    spread_wait(sdb, sd, sdo_s, sdo_r)
    spread_wait(dnb, ed, edo_s, edo_r)


def handed(S, gub, shb, outb, ed, sd, eg, eu, sg, su, mixed, ed_out, sd_out, sem):
    Hc, Sc = S.Hc, S.Sc
    pairs = [
        (gub.at[:, :, pl.ds(0, Hc)], eg), (gub.at[:, :, pl.ds(Hc, Hc)], eu),
        (shb.at[:, :, pl.ds(0, Sc)], sg), (shb.at[:, :, pl.ds(Sc, Sc)], su),
        (outb, mixed), (ed, ed_out), (sd, sd_out),
    ]
    stores = [pltpu.make_async_copy(a, b, sem.at[i]) for i, (a, b) in enumerate(pairs)]
    for copy in stores:
        copy.start()
    for copy in stores:
        copy.wait()


def on_device(
    tokens, norm_gain, gate_train, up_train, down_train,
    shared_gate_train, shared_up_train, shared_down_train, route_expert, route_weight,
):
    S = Sizes(
        lax.axis_size("fs"), lax.axis_size("tp"), tokens.shape, gate_train.shape,
        down_train.shape, shared_gate_train.shape, shared_down_train.shape,
        route_expert.shape[1],
    )
    E, Pn, C, Z, Y = S.E, S.P, S.C, S.Z, S.Y
    T, D, cap, Dr, Hc, Hr, Dc, Sc, Sr, per = (
        S.T, S.D, S.cap, S.Dr, S.Hc, S.Hr, S.Dc, S.Sc, S.Sr, S.per
    )
    dma = pltpu.SemaphoreType.DMA
    anywhere = pl.BlockSpec(memory_space=pl.ANY)
    inside = pl.BlockSpec(memory_space=pltpu.VMEM)
    far = max(1, Y - 1)
    scratch = [
        pltpu.VMEM((T, D), BF16),
        pltpu.VMEM((Z, T, Dc), BF16),
        pltpu.VMEM((Z, 8, T), F32),
        pltpu.VMEM((E, Sr, Dc), BF16),
        pltpu.VMEM((E, Dr, 2 * Hc), BF16),
        pltpu.VMEM((E, Hr, Dc), BF16),
        pltpu.VMEM((E, Hr, Dc), BF16),
        pltpu.VMEM((Pn, E, cap, Dc), BF16),
        pltpu.VMEM((Z, far, cap, Dc), BF16),
        pltpu.VMEM((Z, Y, cap, Dc), BF16),
        pltpu.VMEM((Pn, E, cap, Hc), BF16),
        pltpu.VMEM((E, cap, Dc), BF16),
        pltpu.VMEM((E // 2, cap, Dc), BF16),
        pltpu.VMEM((T, Dc), BF16),
        pltpu.VMEM((T, Dc), F32),
        pltpu.VMEM((Pn, T, Sc), BF16),
        pltpu.VMEM((2, Hr, Dc), F32),
        pltpu.VMEM((Dr, 128), F32),
        dma((2, 3)), dma((1,)), dma((8,)),
        dma((2, Z)), dma((Z,)), dma((Z,)), dma((Z,)),
        dma((2, Z)), dma((E,)), dma((far,)),
        dma((2, Z)), dma((E,)), dma((far,)),
        dma((E,)), dma((E,)), dma((E,)), dma((E,)),
        dma((far,)), dma((Y,)), dma((Pn, E)), dma((C,)), dma((C,)), dma((C,)),
        dma((Pn,)), dma((Pn, S.groups)), dma((Pn,)), dma((Pn,)),
        dma((Pn,)), dma((Pn,)), dma((Pn,)), dma((Pn,)),
        dma((E,)), dma((E,)),
        dma((E // 2,)), dma((1,)), dma((1,)),
    ]
    shape = lambda *dims: jax.ShapeDtypeStruct(dims, BF16)
    flops = 2 * T * D * 2 * Sc + 2 * E * cap * D * 2 * Hc + 4 * E * cap * D * Hc
    vmem = pltpu.MemorySpace.VMEM
    handed_on = [
        (E, Dr, 2 * Hc), (E, Dr, 2 * Sc), (T, Dc), (per, Hr, D), (per, Sr, D)
    ]
    limit = 66781184 - 2 * sum(math.prod(dims) for dims in handed_on)
    outs = pl.pallas_call(
        functools.partial(kernel, S),
        out_shape=[vmem(dims, BF16) for dims in handed_on],
        in_specs=[anywhere] * 7 + [inside] * 3,
        out_specs=[inside] * 5,
        scratch_shapes=scratch,
        compiler_params=pltpu.CompilerParams(
            collective_id=0, has_side_effects=True, vmem_limit_bytes=limit
        ),
        cost_estimate=pl.CostEstimate(flops=flops, bytes_accessed=1 << 26, transcendentals=0),
    )(
        tokens, gate_train, up_train, down_train, shared_gate_train, shared_up_train,
        shared_down_train, norm_gain[None, :], route_expert.T, route_weight.T,
    )
    eg, eu, sg, su, mixed, ed, sd = pl.pallas_call(
        functools.partial(handed, S),
        out_shape=[
            shape(E, Dr, Hc), shape(E, Dr, Hc), shape(E, Dr, Sc), shape(E, Dr, Sc),
            shape(T, Dc), shape(per, Hr, D), shape(per, Sr, D),
        ],
        in_specs=[inside] * 5,
        out_specs=[anywhere] * 7,
        scratch_shapes=[dma((7,))],
        compiler_params=pltpu.CompilerParams(vmem_limit_bytes=1 << 22),
    )(
        *[pltpu.with_memory_space_constraint(o, vmem) for o in outs],
    )
    return (
        eg.reshape(1, D, Hc), eu.reshape(1, D, Hc), ed.reshape(1, per * Hr, D),
        sg.reshape(D, Sc), su.reshape(D, Sc), sd.reshape(per * Sr, D), mixed,
    )


def solution(mesh):
    placed = (
        P("fs", None),
        P("fs"),
        P(None, "fs", "tp"),
        P(None, "fs", "tp"),
        P(None, "fs", "tp"),
        P("fs", "tp"),
        P("fs", "tp"),
        P("fs", "tp"),
        P("fs", None),
        P("fs", None),
    )
    return jax.shard_map(
        on_device,
        mesh=mesh,
        in_specs=placed,
        out_specs=(
            P("fs", None, "tp"),
            P("fs", None, "tp"),
            P("fs", "tp", None),
            P(None, "tp"),
            P(None, "tp"),
            P("tp", None),
            P("fs", "tp"),
        ),
        check_vma=False,
    )
```

```python
import functools
import math

import jax
import jax.numpy as jnp
from jax import lax
from jax.experimental import pallas as pl
from jax.experimental.pallas import tpu as pltpu
from jax.sharding import PartitionSpec as P

norm_eps = 1e-06
cores = 2
MESH = pl.DeviceIdType.MESH
F32, BF16 = jnp.float32, jnp.bfloat16


class Sizes:
    def __init__(self, experts, pieces, tokens, gate, down, sgate, sdown, top):
        self.E, self.P = experts, pieces
        self.C = pieces // cores
        long = 1
        while long * long < experts:
            long *= 2
        self.Z, self.Y = long, experts // long
        self.half = experts // 2
        self.T, self.D = tokens
        self.cap = 3 * self.T * top // (2 * experts)
        self.Dr, self.Hc = gate[1:]
        self.Hr, self.Dc = down[1:]
        self.Dr2, self.Sc = sgate
        self.Sr = sdown[0]
        self.per = experts // pieces
        self.g = 1
        while self.g * self.cap % 128:
            self.g *= 2
        self.groups = experts // self.g
        self.M = self.g * self.cap
        self.nt = min(256, self.Dc)
        assert self.groups <= self.Z and self.M <= self.T


def kernel(
    S,
    tokens, gate_t, up_t, down_t, sgate_t, sup_t, sdown_t, gain, route, weight,
    gub, shb, outb, ed, sd,
    nrm, tok, info, sdb, gst, dst, dnb, rows, yst, est, hid, ret, cmb, farin, acc, shid,
    dbuf, gcol,
    ld_sem, tk_ld, out_sem,
    tok_s, tok_r, info_s, info_r, sh_s, sh_r, shy_s, sd_s, sd_r, sdy_s,
    gu_s, gu_r, dn_s, dn_r, y_s, e_s, rows_r, x_s, part_s, part_r,
    hid_s, hid_r, shid_s, shid_r, edo_s, edo_r, sdo_s, sdo_r, ret_s, ret_r,
    cmb_r, far_s, far_r,
):
    E, Pn, C, Z, Y, half, per = S.E, S.P, S.C, S.Z, S.Y, S.half, S.per
    cap, Dc, Hc, Sc, nt = S.cap, S.Dc, S.Hc, S.Sc, S.nt
    f, t = lax.axis_index("fs"), lax.axis_index("tp")
    z, y = f // Y, f % Y
    x, c = t // cores, t % cores
    inner = (z > 0) & (z < Z - 1)
    to_low, to_high = z == 1, z == Z - 2

    def peer(k):
        span = Z // 2
        p = k // Y
        near = p // span
        plane = (z // span + 1 + near) % 2 * span + (z + p + near) % span
        return plane * Y + (y + 1 + k % Y) % Y

    def rcopy(src, dst, ssem, rsem, to):
        return pltpu.make_async_remote_copy(
            src_ref=src, dst_ref=dst, send_sem=ssem, recv_sem=rsem,
            device_id=to, device_id_type=MESH,
        )

    def arrived(ref, rsem):
        rcopy(ref, ref, out_sem.at[0], rsem, ((f + 1) % E, t)).wait_recv()

    def sent(ref, ssem):
        rcopy(ref, ref, ssem, out_sem.at[0], ((f + 1) % E, t)).wait_send()

    def loop(count, body, start=0):
        lax.fori_loop(start, count, lambda i, v: (body(i), v)[1], 0)

    def passing(slot, i):
        at = pl.multiple_of((slot * 2 + i) * Hc, Hc)
        return acc.at[pl.ds(0, S.Dr), pl.ds(at, Hc)]

    def load_w(k, slot):
        e = peer(k)
        return [
            pltpu.make_async_copy(w.at[e], passing(slot, i), ld_sem.at[slot, i])
            for i, w in ((0, gate_t), (1, up_t))
        ]

    def load_d(k, slot):
        return pltpu.make_async_copy(down_t.at[peer(k)], dbuf.at[slot], ld_sem.at[slot, 2])

    tok_load = pltpu.make_async_copy(tokens, nrm, tk_ld.at[0])
    tok_load.start()
    sh_loads = [
        pltpu.make_async_copy(sgate_t, passing(1, 0), ld_sem.at[1, 0]),
        pltpu.make_async_copy(sup_t, passing(1, 1), ld_sem.at[1, 1]),
        pltpu.make_async_copy(sdown_t, dbuf.at[1], ld_sem.at[1, 2]),
    ]
    for copy in sh_loads + load_w(0, 0) + [load_d(0, 0)]:
        copy.start()
    greet = pltpu.get_barrier_semaphore()
    for i in range(1, E):
        pl.semaphore_signal(greet, inc=1, device_id=((f + i) % E, t), device_id_type=MESH)
    for i in range(1, Pn):
        pl.semaphore_signal(greet, inc=1, device_id=(f, (t + i) % Pn), device_id_type=MESH)

    T = S.T
    gcol[...] = jnp.broadcast_to(gain[...], (128, S.Dr)).T
    for copy in sh_loads:
        copy.wait()
    shb[f, :, 0:Sc] = (gcol[:, 0:1] * passing(1, 0)[...]).astype(BF16)
    shb[f, :, Sc:] = (gcol[:, 0:1] * passing(1, 1)[...]).astype(BF16)
    sdb[f] = dbuf[1].astype(BF16)

    by_z = lambda zs: zs
    by_f = lambda zs: zs * Y + y

    def lanes_of(slot_of, hop, within):
        low, high = (1, Z - 1) if within else (0, Z)
        for d in range(2):
            zs = z - hop if d == 0 else z + hop
            there = (zs >= 0) if d == 0 else (zs < Z)
            if within and hop:
                there &= inner
            onward = (z + 1 < high) if d == 0 else (z > low)
            yield d, there, onward, slot_of(jnp.clip(zs, 0, Z - 1)), f + Y if d == 0 else f - Y

    def line(buf, slot_of, ssem, rsem, hop, within=False):
        for d, there, onward, slot, nxt in lanes_of(slot_of, hop, within):

            @pl.when(there)
            def _():
                if hop:
                    arrived(buf.at[slot], rsem.at[slot])

                @pl.when(onward)
                def _():
                    rcopy(
                        buf.at[slot], buf.at[slot], ssem.at[d, hop], rsem.at[slot], (nxt, t)
                    ).start()

    def line_sent(buf, slot_of, ssem, hop, within=False):
        for d, there, onward, slot, nxt in lanes_of(slot_of, hop, within):

            @pl.when(there & onward)
            def _():
                sent(buf.at[slot], ssem.at[d, hop])


    def shared_y(zs):
        s = by_f(zs)
        for j in range(1, Y):
            to = (z * Y + (y + j) % Y, t)
            rcopy(shb.at[s], shb.at[s], shy_s.at[j - 1], sh_r.at[s], to).start()
            rcopy(sdb.at[s], sdb.at[s], sdy_s.at[j - 1], sd_r.at[s], to).start()

    def come(hop, act_on):
        for zs, there in ((z - hop, z - hop >= 0), (z + hop, z + hop < Z)):
            at = jnp.clip(zs, 0, Z - 1)

            @pl.when(there)
            def _():
                act_on(at)

    def shared_hop(hop):
        line(shb, by_f, sh_s, sh_r, hop)
        line(sdb, by_f, sd_s, sd_r, hop)
        if hop:
            come(hop, shared_y)
        else:
            shared_y(z)

    pl.semaphore_wait(greet, E + Pn - 2)
    shared_hop(0)
    wide = max(16, E)
    r0, r1 = route[0:1, :].astype(F32), route[1:2, :].astype(F32)
    names = lax.broadcasted_iota(jnp.int32, (wide, T), 0).astype(F32)
    hit0, hit1 = r0 == names, r1 == names
    chosen = (hit0 | hit1).astype(F32).astype(BF16)
    before = lax.broadcasted_iota(jnp.int32, (T, T), 0) < lax.broadcasted_iota(
        jnp.int32, (T, T), 1
    )
    count = jnp.dot(chosen, before.astype(F32).astype(BF16), preferred_element_type=F32)
    s0 = jnp.sum(jnp.where(hit0, count, 0.0), axis=0, keepdims=True)
    s1 = jnp.sum(jnp.where(hit1, count, 0.0), axis=0, keepdims=True)
    info[z, 0:1, :] = r0
    info[z, 1:2, :] = r1
    info[z, 2:3, :] = s0
    info[z, 3:4, :] = s1
    info[z, 4:6, :] = weight[...]

    tok_load.wait()
    tile = min(64, T)

    def normalise(i):
        at = pl.ds(pl.multiple_of(i * tile, tile), tile)
        v = nrm[at, :].astype(F32)
        v = v * lax.rsqrt(jnp.mean(v * v, axis=1, keepdims=True) + norm_eps)
        nrm[at, :] = v.astype(BF16)
        tok[z, at, :] = nrm[at, pl.ds(pl.multiple_of(t * Dc, Dc), Dc)]

    loop(T // tile, normalise)

    def tell(act_on):
        for i in range(1, Z):
            zo = (z + i) % Z

            @pl.when((zo > 0) & (zo < Z - 1))
            def _():
                act_on(i - 1, zo)

    tell(
        lambda i, zo: rcopy(
            info.at[z], info.at[z], info_s.at[i], info_r.at[z], (zo * Y + y, t)
        ).start()
    )
    line(tok, by_z, tok_s, tok_r, 0, True)

    def convert_gu(k):
        slot = k % 2
        for copy in load_w(k, slot):
            copy.wait()

        @pl.when(k + 1 < E)
        def _():
            for copy in load_w(k + 1, 1 - slot):
                copy.start()

        for i in range(2):
            gst[k, :, i * Hc : (i + 1) * Hc] = (gcol[:, 0:1] * passing(slot, i)[...]).astype(BF16)

    def convert_dn(k):
        slot = k % 2
        load_d(k, slot).wait()

        @pl.when(k + 1 < E)
        def _():
            load_d(k + 1, 1 - slot).start()

        dst[k] = dbuf[slot].astype(BF16)

    def x_out(s):
        for i in range(1, C):
            to = (f, (x + i) % C * cores + c)
            rcopy(rows.at[t, s], rows.at[t, s], x_s.at[i - 1], rows_r.at[t, s], to).start()
        rcopy(rows.at[t, s], rows.at[t, s], part_s.at[0], part_r.at[0], (f, x * cores + 1 - c)).start()

    def picked(zs, e, put_block):
        e = e.astype(F32)
        slots = lax.broadcasted_iota(jnp.int32, (cap, T), 0).astype(F32)
        got = (info[zs, 0:1, :] == e) & (info[zs, 2:3, :] == slots)
        got |= (info[zs, 1:2, :] == e) & (info[zs, 3:4, :] == slots)
        got = got.astype(F32).astype(BF16)

        def part(n):
            at = pl.ds(pl.multiple_of(n * nt, nt), nt)
            put_block(at, jnp.dot(got, tok[zs, :, at], preferred_element_type=F32).astype(BF16))

        loop(Dc // nt, part)

    def pick(zs):
        s = by_f(zs)

        def for_end(zt):
            for j in range(Y):

                def put_block(at, block):
                    est[zs, j, :, at] = block

                picked(zs, zt * Y + (y + j) % Y, put_block)
            for j in range(Y):
                rcopy(
                    est.at[zs, j], rows.at[t, s], e_s.at[j], rows_r.at[t, s],
                    (zt * Y + (y + j) % Y, t),
                ).start()

        for zt, near in ((0, to_low), (Z - 1, to_high)):

            @pl.when(near & (zs != zt))
            def _():
                for_end(zt)

        for j in list(range(1, Y)) + [0]:

            def put_block(at, block):
                if j:
                    yst[zs, j - 1, :, at] = block
                else:
                    rows[t, s, :, at] = block

            picked(zs, z * Y + (y + j) % Y, put_block)
        for j in range(1, Y):
            to = (z * Y + (y + j) % Y, t)
            rcopy(
                yst.at[zs, j - 1], rows.at[t, s], y_s.at[j - 1], rows_r.at[t, s], to
            ).start()
        x_out(s)

    def send_gu(k):
        e = peer(k)
        rcopy(gst.at[k], gub.at[f], gu_s.at[k], gu_r.at[f], (e, t)).start()

    def send_dn(k):
        e = peer(k)
        rcopy(dst.at[k], dnb.at[f], dn_s.at[k], dn_r.at[f], (e, t)).start()

    def pick_come(at):
        arrived(info.at[at], info_r.at[at])
        pick(at)

    def tok_hop(hop):
        line(tok, by_z, tok_s, tok_r, hop, True)

        @pl.when(inner)
        def _():
            come(hop, pick_come)

    pick(z)
    loop(E, convert_gu)
    loop(E, convert_dn)
    gub[f] = gst[E - 1]
    dnb[f] = dst[E - 1]
    for hop in range(1, Z - 1):
        tok_hop(hop)
        shared_hop(hop)
        line_sent(tok, by_z, tok_s, hop - 1, True)
        line_sent(shb, by_f, sh_s, hop - 1)
        line_sent(sdb, by_f, sd_s, hop - 1)
    if Z == 2:
        line_sent(tok, by_z, tok_s, 0, True)
        line_sent(shb, by_f, sh_s, 0)
        line_sent(sdb, by_f, sd_s, 0)
    if Z > 2:
        line_sent(tok, by_z, tok_s, Z - 2, True)
    loop(half // 2, send_gu)
    loop(E - 1, send_gu, half)

    for i in range(Z):
        zs = jnp.where(z < Z // 2, z + i, z + Z - i) % Z
        for j in range(Y):
            s = zs * Y + (y + j) % Y
            if j:
                arrived(rows.at[t, s], rows_r.at[t, s])
                x_out(s)
            elif i:

                @pl.when(jnp.logical_not(inner))
                def _():
                    arrived(rows.at[t, s], rows_r.at[t, s])
                    x_out(s)

    loop(half // 2, lambda k: sent(gst.at[k], gu_s.at[k]))
    loop(half, send_gu, half // 2)
    loop(E - 1, send_dn, half)
    for i in range(1, C):
        to_t = (x + i) % C * cores + c

        def forward(s):
            arrived(rows.at[to_t, s], rows_r.at[to_t, s])
            rcopy(
                rows.at[to_t, s], rows.at[to_t, s], part_s.at[i], part_r.at[i],
                (f, x * cores + 1 - c),
            ).start()

        loop(E, forward)
    own_cols = pl.ds(pl.multiple_of(t * Dc, Dc), Dc)

    def spread(buf, out, ssem, rsem):
        for k in range(1, Pn):
            tt = (t + k) % Pn
            rcopy(
                buf.at[pl.ds(tt * per, per)], out.at[:, :, own_cols], ssem.at[k - 1],
                rsem.at[t], (f, tt),
            ).start()
        out[:, :, own_cols] = buf[pl.ds(t * per, per)]

    def spread_wait(buf, out, ssem, rsem):
        for k in range(1, Pn):
            tt = (t + k) % Pn
            sent(buf.at[pl.ds(tt * per, per)], ssem.at[k - 1])
            at = pl.ds(pl.multiple_of(tt * Dc, Dc), Dc)
            arrived(out.at[:, :, at], rsem.at[tt])

    if Z > 2:
        shared_hop(Z - 1)
    loop(half, lambda k: sent(gst.at[k], gu_s.at[k]), half // 2)

    @pl.when(inner)
    def _():
        loop(half, send_dn)


    def act(v, width):
        gate, up = v[:, :width], v[:, width:]
        return (gate / (1.0 + jnp.exp(-gate)) * up).astype(BF16)

    mt = min(256, T)

    def shared_in(m):
        at = pl.ds(pl.multiple_of(m * mt, mt), mt)
        total = None
        for q in range(Pn):
            w = shb[q * per : (q + 1) * per].reshape(Dc, 2 * Sc)
            term = jnp.dot(nrm[at, q * Dc : (q + 1) * Dc], w, preferred_element_type=F32)
            total = term if total is None else total + term
        shid[t, at, :] = act(total, Sc)

    def inner_of(s):
        return (s // Y > 0) & (s // Y < Z - 1)

    def rows_waits():
        part = x * cores + 1 - c
        arrived(rows.at[part], part_r.at[0])
        for i in range(1, C):
            arrived(rows.at[(x + i) % C * cores + 1 - c], part_r.at[i])

    rows_waits()

    def wait_gu(k):
        s = peer(k)
        arrived(gub.at[s], gu_r.at[s])

    loop(E - 1, wait_gu)

    @pl.when(jnp.logical_not(inner))
    def _():
        loop(half, send_dn)

    M, g, groups = S.M, S.g, S.groups
    own = f // g

    low = f < half
    side = groups // 2
    mid_z = jnp.where(low, Z // 2 - 1, Z // 2)
    over_z = jnp.where(low, Z // 2, Z // 2 - 1)

    def group_at(k):
        at = jnp.where(inner, k, side - 1 - k)
        far = jnp.where(low, groups - 1 - at, at)
        near = own // side * side + (own + 1 + k - side) % side
        return jnp.where(k < side, far, near)

    def hidden_in(k):
        q0 = group_at(k)
        span = pl.ds(q0 * g, g)
        total = None
        for q in range(Pn):
            w = gub[q * per : (q + 1) * per].reshape(Dc, 2 * Hc)
            term = jnp.dot(rows[q, span].reshape(M, Dc), w, preferred_element_type=F32)
            total = term if total is None else total + term
        hid[t, span] = act(total, Hc).reshape(g, cap, Hc)

    partner = x * cores + 1 - c

    def pass_hidden(i, tt, k, to):
        span = pl.ds(group_at(k) * g, g)
        rcopy(hid.at[tt, span], hid.at[tt, span], hid_s.at[i], hid_r.at[tt, k], (f, to)).start()

    def send_hidden(k):
        for i in range(1, C):
            pass_hidden(i, t, k, (x + i) % C * cores + c)
        pass_hidden(0, t, k, partner)

    def forward_hidden(k):
        span = pl.ds(group_at(k) * g, g)
        for i in range(1, C):
            tt = (x + i) % C * cores + c
            arrived(hid.at[tt, span], hid_r.at[tt, k])
            pass_hidden(C - 1 + i, tt, k, partner)

    def hidden_step(k):
        hidden_in(k)

        @pl.when(k > 0)
        def _():
            send_hidden(k - 1)

    loop(groups, hidden_step)

    def wait_dn(k):
        s = peer(k)
        arrived(dnb.at[s], dn_r.at[s])

    send_hidden(groups - 1)
    for j in range(1, Y):
        for zs in range(Z):
            s = zs * Y + (y + j) % Y
            arrived(shb.at[s], sh_r.at[s])
            arrived(sdb.at[s], sd_r.at[s])

    loop(T // mt, shared_in)

    for k in range(1, Pn):
        rcopy(shid.at[t], shid.at[t], shid_s.at[k - 1], shid_r.at[t], (f, (t + k) % Pn)).start()
    spread(sdb, sd, sdo_s, sdo_r)
    loop(groups, forward_hidden)
    loop(E - 1, wait_dn)

    def res_at(s):
        return tok.at[s // g, pl.ds(pl.multiple_of(s % g * cap, cap), cap)]

    def send_back(k):
        for i in range(g):
            s = group_at(k) * g + i
            over = (s // Y == over_z) & inner_of(s)
            to = mid_z * Y + s % Y

            @pl.when(over & (to != f))
            def _():
                rcopy(res_at(s), cmb.at[f % half], ret_s.at[s], cmb_r.at[f % half], (to, t)).start()

            @pl.when(jnp.logical_not(over) & (s != f))
            def _():
                rcopy(res_at(s), ret.at[f], ret_s.at[s], ret_r.at[f], (s, t)).start()

    def back_step(k):
        span = pl.ds(group_at(k) * g, g)

        for i in range(C):
            tt = (x + i) % C * cores + 1 - c
            arrived(hid.at[tt, span], hid_r.at[tt, k])

        def part(n):
            at = pl.ds(pl.multiple_of(n * nt, nt), nt)
            total = None
            for q in range(Pn):
                w = dnb[q * per : (q + 1) * per, :, at].reshape(Hc, nt)
                term = jnp.dot(hid[q, span].reshape(M, Hc), w, preferred_element_type=F32)
                total = term if total is None else total + term
            tok[group_at(k), 0:M, at] = total.astype(BF16)

        loop(Dc // nt, part)
        send_back(k)

    loop(groups, back_step)
    ret[f] = res_at(f)[...]

    def weigh(zs, base, many):
        spot = (lax.broadcasted_iota(jnp.int32, (many, T), 0) + base).astype(F32)
        at0 = info[zs, 0:1, :] * cap + info[zs, 2:3, :]
        at1 = info[zs, 1:2, :] * cap + info[zs, 3:4, :]
        share = jnp.where(at0 == spot, info[zs, 4:5, :], 0.0)
        share += jnp.where(at1 == spot, info[zs, 5:6, :], 0.0)
        return share.T.astype(BF16)

    spread(dnb, ed, edo_s, edo_r)
    @pl.when(inner)
    def _():
        to = over_z * Y + y
        cmb[f % half] = res_at(to)[...]
        many = half * cap
        shares = weigh(over_z, f // half * many, many)
        for i in range(1, half):
            e = (f + i) % half
            arrived(cmb.at[e], cmb_r.at[e])

        def part(n):
            at = pl.ds(pl.multiple_of(n * nt, nt), nt)
            block = cmb[:, :, at].reshape(many, nt)
            nrm[:, at] = jnp.dot(shares, block, preferred_element_type=F32).astype(BF16)

        loop(Dc // nt, part)
        rcopy(nrm.at[:, pl.ds(0, Dc)], farin, far_s.at[0], far_r.at[0], (to, t)).start()


    for k in range(1, Pn):
        arrived(shid.at[(t + k) % Pn], shid_r.at[(t + k) % Pn])

    def shared_out(n):
        at = pl.ds(pl.multiple_of(n * nt, nt), nt)
        total = None
        for q in range(Pn):
            w = sdb[q * per : (q + 1) * per, :, at].reshape(Sc, nt)
            term = jnp.dot(shid[q], w, preferred_element_type=F32)
            total = term if total is None else total + term
        acc[:, at] = total

    loop(Dc // nt, shared_out)


    def combine(k):
        q0 = group_at(groups - 1 - k)
        shares = weigh(z, q0 * M, M)
        for j in range(g):
            s = q0 * g + j

            @pl.when(s != f)
            def _():
                arrived(ret.at[s], ret_r.at[s])


        def part(n):
            at = pl.ds(pl.multiple_of(n * nt, nt), nt)
            block = ret[pl.ds(q0 * g, g), :, at].reshape(M, nt)
            acc[:, at] += jnp.dot(shares, block, preferred_element_type=F32)

        loop(Dc // nt, part)

    if Z > 2:
        line_sent(shb, by_f, sh_s, Z - 2)
        line_sent(sdb, by_f, sd_s, Z - 2)
    tell(lambda i, zo: sent(info.at[z], info_s.at[i]))
    for j in range(1, Y):
        sent(shb.at[pl.ds(0, Z)], shy_s.at[j - 1])
        sent(sdb.at[pl.ds(0, Z)], sdy_s.at[j - 1])

        @pl.when(inner)
        def _():
            sent(yst.at[:, j - 1], y_s.at[j - 1])

        @pl.when(jnp.logical_not(inner))
        def _():
            sent(yst.at[0, j - 1], y_s.at[j - 1])

    @pl.when(to_low | to_high)
    def _():
        for j in range(Y):
            sent(est.at[pl.ds(0, Z - 1), j], e_s.at[j])

    for i in range(1, C):
        sent(rows.at[t], x_s.at[i - 1])
    for i in range(C):
        sent(rows.at[t], part_s.at[i])
    loop(E - 1, lambda k: sent(gst.at[k], gu_s.at[k]), half)
    loop(E - 1, lambda k: sent(dst.at[k], dn_s.at[k]))
    loop(side, combine)

    @pl.when(jnp.logical_not(inner))
    def _():
        loop(groups, combine, side)
        outb[...] = acc[...].astype(BF16)

    @pl.when(inner)
    def _():
        arrived(farin, far_r.at[0])
        outb[...] = (acc[...] + farin[...].astype(F32)).astype(BF16)


    for k in range(1, Pn):
        sent(shid.at[t], shid_s.at[k - 1])
        sent(hid.at[t], hid_s.at[k - 1])

    def drain_ret(k):
        s = peer(k)

        @pl.when(jnp.logical_not(inner & (s == over_z * Y + y)))
        def _():
            sent(res_at(s), ret_s.at[s])

    @pl.when(inner)
    def _():
        sent(nrm.at[:, pl.ds(0, Dc)], far_s.at[0])

    loop(E - 1, drain_ret)
    spread_wait(sdb, sd, sdo_s, sdo_r)
    spread_wait(dnb, ed, edo_s, edo_r)


def handed(S, gub, shb, outb, ed, sd, eg, eu, sg, su, mixed, ed_out, sd_out, sem):
    Hc, Sc = S.Hc, S.Sc
    pairs = [
        (gub.at[:, :, pl.ds(0, Hc)], eg), (gub.at[:, :, pl.ds(Hc, Hc)], eu),
        (shb.at[:, :, pl.ds(0, Sc)], sg), (shb.at[:, :, pl.ds(Sc, Sc)], su),
        (outb, mixed), (ed, ed_out), (sd, sd_out),
    ]
    stores = [pltpu.make_async_copy(a, b, sem.at[i]) for i, (a, b) in enumerate(pairs)]
    for copy in stores:
        copy.start()
    for copy in stores:
        copy.wait()


def on_device(
    tokens, norm_gain, gate_train, up_train, down_train,
    shared_gate_train, shared_up_train, shared_down_train, route_expert, route_weight,
):
    S = Sizes(
        lax.axis_size("fs"), lax.axis_size("tp"), tokens.shape, gate_train.shape,
        down_train.shape, shared_gate_train.shape, shared_down_train.shape,
        route_expert.shape[1],
    )
    E, Pn, C, Z, Y = S.E, S.P, S.C, S.Z, S.Y
    T, D, cap, Dr, Hc, Hr, Dc, Sc, Sr, per = (
        S.T, S.D, S.cap, S.Dr, S.Hc, S.Hr, S.Dc, S.Sc, S.Sr, S.per
    )
    dma = pltpu.SemaphoreType.DMA
    anywhere = pl.BlockSpec(memory_space=pl.ANY)
    inside = pl.BlockSpec(memory_space=pltpu.VMEM)
    far = max(1, Y - 1)
    scratch = [
        pltpu.VMEM((T, D), BF16),
        pltpu.VMEM((Z, T, Dc), BF16),
        pltpu.VMEM((Z, 8, T), F32),
        pltpu.VMEM((E, Sr, Dc), BF16),
        pltpu.VMEM((E, Dr, 2 * Hc), BF16),
        pltpu.VMEM((E, Hr, Dc), BF16),
        pltpu.VMEM((E, Hr, Dc), BF16),
        pltpu.VMEM((Pn, E, cap, Dc), BF16),
        pltpu.VMEM((Z, far, cap, Dc), BF16),
        pltpu.VMEM((Z, Y, cap, Dc), BF16),
        pltpu.VMEM((Pn, E, cap, Hc), BF16),
        pltpu.VMEM((E, cap, Dc), BF16),
        pltpu.VMEM((E // 2, cap, Dc), BF16),
        pltpu.VMEM((T, Dc), BF16),
        pltpu.VMEM((T, Dc), F32),
        pltpu.VMEM((Pn, T, Sc), BF16),
        pltpu.VMEM((2, Hr, Dc), F32),
        pltpu.VMEM((Dr, 128), F32),
        dma((2, 3)), dma((1,)), dma((8,)),
        dma((2, Z)), dma((Z,)), dma((Z,)), dma((Z,)),
        dma((2, Z)), dma((E,)), dma((far,)),
        dma((2, Z)), dma((E,)), dma((far,)),
        dma((E,)), dma((E,)), dma((E,)), dma((E,)),
        dma((far,)), dma((Y,)), dma((Pn, E)), dma((C,)), dma((C,)), dma((C,)),
        dma((Pn,)), dma((Pn, S.groups)), dma((Pn,)), dma((Pn,)),
        dma((Pn,)), dma((Pn,)), dma((Pn,)), dma((Pn,)),
        dma((E,)), dma((E,)),
        dma((E // 2,)), dma((1,)), dma((1,)),
    ]
    shape = lambda *dims: jax.ShapeDtypeStruct(dims, BF16)
    flops = 2 * T * D * 2 * Sc + 2 * E * cap * D * 2 * Hc + 4 * E * cap * D * Hc
    vmem = pltpu.MemorySpace.VMEM
    handed_on = [
        (E, Dr, 2 * Hc), (E, Dr, 2 * Sc), (T, Dc), (per, Hr, D), (per, Sr, D)
    ]
    limit = 66781184 - 2 * sum(math.prod(dims) for dims in handed_on)
    outs = pl.pallas_call(
        functools.partial(kernel, S),
        out_shape=[vmem(dims, BF16) for dims in handed_on],
        in_specs=[anywhere] * 7 + [inside] * 3,
        out_specs=[inside] * 5,
        scratch_shapes=scratch,
        compiler_params=pltpu.CompilerParams(
            collective_id=0, has_side_effects=True, vmem_limit_bytes=limit
        ),
        cost_estimate=pl.CostEstimate(flops=flops, bytes_accessed=1 << 26, transcendentals=0),
    )(
        tokens, gate_train, up_train, down_train, shared_gate_train, shared_up_train,
        shared_down_train, norm_gain[None, :], route_expert.T, route_weight.T,
    )
    eg, eu, sg, su, mixed, ed, sd = pl.pallas_call(
        functools.partial(handed, S),
        out_shape=[
            shape(E, Dr, Hc), shape(E, Dr, Hc), shape(E, Dr, Sc), shape(E, Dr, Sc),
            shape(T, Dc), shape(per, Hr, D), shape(per, Sr, D),
        ],
        in_specs=[inside] * 5,
        out_specs=[anywhere] * 7,
        scratch_shapes=[dma((7,))],
        compiler_params=pltpu.CompilerParams(vmem_limit_bytes=1 << 22),
    )(
        *[pltpu.with_memory_space_constraint(o, vmem) for o in outs],
    )
    return (
        eg.reshape(1, D, Hc), eu.reshape(1, D, Hc), ed.reshape(1, per * Hr, D),
        sg.reshape(D, Sc), su.reshape(D, Sc), sd.reshape(per * Sr, D), mixed,
    )


def solution(mesh):
    placed = (
        P("fs", None),
        P("fs"),
        P(None, "fs", "tp"),
        P(None, "fs", "tp"),
        P(None, "fs", "tp"),
        P("fs", "tp"),
        P("fs", "tp"),
        P("fs", "tp"),
        P("fs", None),
        P("fs", None),
    )
    return jax.shard_map(
        on_device,
        mesh=mesh,
        in_specs=placed,
        out_specs=(
            P("fs", None, "tp"),
            P("fs", None, "tp"),
            P("fs", "tp", None),
            P(None, "tp"),
            P(None, "tp"),
            P("tp", None),
            P("fs", "tp"),
        ),
        check_vma=False,
    )
```
